512 devices in a mesh: sp: 16 (over y, x), tp: 32 (over z, core).
Axes of the slice: x: 4, y: 4, z: 16, core: 2. Of those that a mesh axis runs over, the one named last changes fastest.
Arguments:
- tokens: bfloat16 [3, 8192, 4096], P(None, 'sp', 'tp'), may hold values from -6 to 6
- new_token: bfloat16 [3, 1, 4096], P(None, None, 'tp'), may hold values from -6 to 6
- query_weight: bfloat16 [4096, 4096], P(None, 'tp'), may hold values from -0.09375 to 0.09375
- key_weight: bfloat16 [4096, 4096], P(None, 'tp'), may hold values from -0.09375 to 0.09375
- value_weight: bfloat16 [4096, 4096], P(None, 'tp'), may hold values from -0.09375 to 0.09375
- log_decay: float32 [64], P('tp'), may hold values from -0.034 to 0
Outputs:
- state: bfloat16 [3, 64, 64, 64], P(None, 'tp', 'sp')
- read: bfloat16 [3, 4096], P(None, 'tp')
The draws below stay inside these ranges and needn't reach their ends.
All inputs are finite; a program needn't handle non-finite values.
Results may differ from the reference program's by a relative error of at most 0.012.
Values may be sent and summed in bfloat16 or wider, within the bound.
No kernel may reach another device: no remote copies, remote signals or barrier semaphores. Data moves between devices by JAX's collectives and lax.ppermute only.
A program may use at most 64 MiB of HBM per device.

```python
import jax
import jax.numpy as jnp
from jax import lax

D = 4096
HEADS = 64
HD = 64
SEQS = 3
SPAN = 512
LEN = 8192
N_SP = 16


def draw_log_decay(key, part):
    choose_key = jax.random.fold_in(key, 11)
    fast_key = jax.random.fold_in(key, 12)
    slow_key = jax.random.fold_in(key, 13)
    chain_len = max(LEN, 64)
    fast_heads = jax.random.randint(choose_key, (HEADS,), 0, 2) == 1
    slow_rates = -jax.random.uniform(slow_key, (HEADS,), jnp.float32, 0.1, 2.0) / chain_len
    fast_rates = -1.0 / jax.random.uniform(fast_key, (HEADS,), jnp.float32, 30.0, 100.0)
    return jnp.where(fast_heads, fast_rates, slow_rates).astype(jnp.float32)


def shard_levels(own_key, dims, shards, low, top_value):
    def one(axis_at, parts):
        heights = jax.random.uniform(jax.random.fold_in(jax.random.fold_in(own_key, 6), axis_at), (parts,), jnp.float32, low / len(shards), top_value / len(shards))
        return jnp.repeat(jnp.exp(heights), dims[axis_at] // parts).reshape((-1,) + (1,) * (len(dims) - axis_at - 1))

    loudness = one(*shards[0])
    for cut in shards[1:]:
        loudness = loudness * one(*cut)
    return loudness


def bell_draw(rng, shape, spread, bound, pieces=(), kind=jnp.bfloat16):
    drawn = jax.random.normal(rng, shape, jnp.float32) * spread
    if len(pieces) > 0:
        drawn = shard_levels(rng, shape, pieces, -0.22, 0.18) * drawn
    return jnp.clip(drawn, min=-bound, max=bound).astype(kind)


def setup_inputs(seed: int = 0) -> dict:
    streams_of = jax.random.split(jax.random.key(seed), 7)
    return {
        "tokens": bell_draw(streams_of[0], (SEQS, LEN, D), 1.0, 6.0, ((1, 16), (2, 32))),
        "new_token": bell_draw(streams_of[1], (SEQS, 1, D), 1.0, 6.0, ((2, 32),)),
        "query_weight": bell_draw(streams_of[2], (D, HEADS * HD), D ** -0.5, 0.09375, ((1, 32),)),
        "key_weight": bell_draw(streams_of[3], (D, HEADS * HD), D ** -0.5, 0.09375, ((1, 32),)),
        "value_weight": bell_draw(streams_of[4], (D, HEADS * HD), D ** -0.5, 0.09375, ((1, 32),)),
        "log_decay": draw_log_decay(jax.random.fold_in(streams_of[6], 71), 0),
    }


def rotate(values, positions):
    half_dim = values.shape[-1] // 2
    inverse = 10000.0 ** (-jnp.arange(half_dim, dtype=jnp.float32) / half_dim)
    angles = positions.astype(jnp.float32)[:, None, None] * inverse[None, None, :]
    cosine = jnp.cos(angles)
    sine_part = jnp.sin(angles)
    first = values[..., :half_dim]
    second = values[..., half_dim:]
    return jnp.concatenate([first * cosine - second * sine_part, first * sine_part + second * cosine], axis=-1)

def group_norm(output):
    centered = output - lax.optimization_barrier(jnp.mean(output, axis=-1, keepdims=True))
    return centered * lax.rsqrt(lax.optimization_barrier(jnp.mean(centered * centered, axis=-1, keepdims=True)) + 1e-05)

def reference(tokens, new_token, query_weight, key_weight, value_weight, log_decay):
    key_scale = HD ** (-0.5)
    positions = jnp.arange(LEN, dtype=jnp.int32)
    to_end = (SPAN - 1 - positions % SPAN).astype(jnp.float32)
    block_ids = jnp.arange(N_SP, dtype=jnp.float32)
    new_position = jnp.full((1,), LEN, jnp.int32)
    query_heads = query_weight.reshape(D, HEADS, HD).transpose(1, 0, 2)
    key_heads = key_weight.reshape(D, HEADS, HD).transpose(1, 0, 2)
    value_heads = value_weight.reshape(D, HEADS, HD).transpose(1, 0, 2)

    def single_head(inputs):
        w_query, w_key, w_value, logarithm_rate = inputs
        projected = jnp.dot(tokens, w_key, preferred_element_type=jnp.float32)[:, :, None, :]
        key_rows = (rotate(projected, positions) * key_scale).astype(jnp.bfloat16)[:, :, 0, :]
        value_rows = jnp.dot(tokens, w_value, preferred_element_type=jnp.float32).astype(jnp.bfloat16)
        weighted = (key_rows.astype(jnp.float32) * jnp.exp(logarithm_rate * to_end)[None, :, None]).astype(jnp.bfloat16)
        weighted = weighted.astype(jnp.float32).reshape(SEQS, N_SP, SPAN, HD)
        value_blocks = value_rows.astype(jnp.float32).reshape(SEQS, N_SP, SPAN, HD)
        segment_states = jnp.einsum('sbtk,sbtv->sbkv', weighted, value_blocks, precision=lax.Precision.HIGHEST)
        carried_state = jnp.exp(logarithm_rate * SPAN * (N_SP - 1 - block_ids))
        closing_state = jnp.einsum('eyzt,y->ezt', segment_states, carried_state, precision=lax.Precision.HIGHEST)
        new_query = rotate(jnp.dot(new_token, w_query, preferred_element_type=jnp.float32)[:, :, None, :], new_position)
        new_query = new_query.astype(jnp.bfloat16)[:, 0, 0, :]
        fresh_key = rotate(jnp.dot(new_token, w_key, preferred_element_type=jnp.float32)[:, :, None, :], new_position)
        fresh_key = (fresh_key * key_scale).astype(jnp.bfloat16)[:, 0, 0, :]
        new_value = jnp.dot(new_token, w_value, preferred_element_type=jnp.float32).astype(jnp.bfloat16)[:, 0, :]
        query_entries = new_query.astype(jnp.float32)
        unscaled_read = jnp.exp(logarithm_rate) * jnp.einsum('bol,bo->bl', closing_state, query_entries, precision=lax.Precision.HIGHEST)
        unscaled_read = unscaled_read + lax.optimization_barrier(jnp.sum(query_entries * fresh_key.astype(jnp.float32), axis=-1, keepdims=True)) * new_value.astype(jnp.float32)
        return (closing_state.astype(jnp.bfloat16), group_norm(unscaled_read).astype(jnp.bfloat16))
    states, reads = lax.map(single_head, (query_heads, key_heads, value_heads, log_decay))
    return (states.transpose(1, 0, 2, 3), reads.transpose(1, 0, 2).reshape(SEQS, HEADS * HD))
```

```python
import jax
import jax.numpy as jnp
from jax import lax
from jax.sharding import PartitionSpec as P

HD = 64


def rotate(values, positions):
    half_dim = values.shape[-1] // 2
    inverse = 10000.0 ** (-jnp.arange(half_dim, dtype=jnp.float32) / half_dim)
    angles = positions.astype(jnp.float32)[:, None, None] * inverse[None, None, :]
    cosine = jnp.cos(angles)
    sine_part = jnp.sin(angles)
    first = values[..., :half_dim]
    second = values[..., half_dim:]
    return jnp.concatenate(
        [first * cosine - second * sine_part, first * sine_part + second * cosine], axis=-1
    )


def group_norm(output):
    centered = output - jnp.mean(output, axis=-1, keepdims=True)
    return centered * lax.rsqrt(jnp.mean(centered * centered, axis=-1, keepdims=True) + 1e-05)


def exchange_sum(value, axis_pairs, own, count):
    total = lax.dynamic_index_in_dim(value, own, 0, keepdims=False)
    arrived = []
    for shift in range(1, count):
        piece = lax.dynamic_index_in_dim(value, (own + shift) % count, 0, keepdims=False)
        arrived.append(lax.ppermute(piece, "sp", axis_pairs[shift]))
    for piece in arrived:
        total = total + piece
    return total


def body(tokens, new_token, query_weight, key_weight, value_weight, log_decay):
    sequences, span_len, width = tokens.shape
    own_heads = log_decay.shape[0]
    groups = lax.axis_size("sp")
    planes = lax.axis_size("tp") // 2
    side = 4
    own_index = lax.axis_index("sp")
    tp_index = lax.axis_index("tp")
    plane = tp_index // 2
    core = tp_index % 2
    key_scale = HD ** (-0.5)
    half = span_len // 2
    rows = sequences * half
    extra = 16

    partner = [(i, i ^ 1) for i in range(2 * planes)]
    up = [(2 * z + c, 2 * ((z + 1) % planes) + c) for z in range(planes) for c in range(2)]
    down = [(2 * z + c, 2 * ((z - 1) % planes) + c) for z in range(planes) for c in range(2)]

    fresh = jnp.concatenate(
        [new_token[:, 0], jnp.zeros((extra - sequences, width), new_token.dtype)], axis=0
    )

    def chunk(which):
        part = lax.dynamic_slice_in_dim(tokens, which * half, half, 1).reshape(rows, width)
        return jnp.concatenate([part, fresh], axis=0)

    first = chunk(core)
    second = lax.ppermute(chunk(1 - core), "tp", partner)

    key_other = lax.ppermute(key_weight, "tp", partner)
    value_other = lax.ppermute(value_weight, "tp", partner)
    decay_other = lax.ppermute(log_decay, "tp", partner)
    row_weights = jnp.concatenate([key_weight, key_other, value_weight, value_other], axis=1)

    def ordered(weights):
        blocks = weights.reshape(planes, 2, width, weights.shape[1])
        blocks = jnp.where(core == 0, blocks, blocks[:, ::-1])
        return blocks.reshape(planes, 2 * width, weights.shape[1])

    row_weights = ordered(row_weights)
    query_rows = ordered(query_weight)

    def project(a, b, offset):
        at = (plane + offset) % planes
        both = jnp.concatenate([a, b], axis=1)
        main = jnp.dot(
            both,
            lax.dynamic_index_in_dim(row_weights, at, 0, keepdims=False),
            preferred_element_type=jnp.float32,
        )
        query = jnp.dot(
            both[rows:],
            lax.dynamic_index_in_dim(query_rows, at, 0, keepdims=False),
            preferred_element_type=jnp.float32,
        )
        return main, query

    main, query = project(first, second, 0)
    up_a = down_a = first
    up_b = down_b = second
    reach = planes // 2
    for step in range(1, reach + 1):
        up_a = lax.ppermute(up_a, "tp", up)
        down_b = lax.ppermute(down_b, "tp", down)
        if step < reach:
            up_b = lax.ppermute(up_b, "tp", up)
            down_a = lax.ppermute(down_a, "tp", down)
            pieces = [(up_a, up_b, -step), (down_a, down_b, step)]
        else:
            pieces = [(up_a, down_b, reach)]
        for a, b, offset in pieces:
            more, more_query = project(a, b, offset)
            main = main + more
            query = query + more_query

    heads = 2 * own_heads
    inner = heads * HD
    decay = jnp.concatenate([log_decay, decay_other])
    key_rows = main[:rows, :inner].reshape(sequences, half, heads, HD)
    value_rows = main[:rows, inner:].reshape(sequences, half, heads, HD).astype(jnp.bfloat16)
    local = core * half + jnp.arange(half, dtype=jnp.int32)
    key_rows = (rotate(key_rows, own_index * span_len + local) * key_scale).astype(jnp.bfloat16)
    to_end = (span_len - 1 - local).astype(jnp.float32)
    decay_rows = jnp.exp(to_end[:, None] * decay[None, :])
    weighted = (key_rows.astype(jnp.float32) * decay_rows[None, :, :, None]).astype(jnp.bfloat16)
    span_state = jnp.einsum(
        "sthk,sthv->shkv", weighted, value_rows, preferred_element_type=jnp.float32
    )
    carried = jnp.exp(decay * (span_len * (groups - 1 - own_index)).astype(jnp.float32))
    scaled = span_state * carried[None, :, None, None]
    state = scaled[:, :own_heads] + lax.ppermute(scaled[:, own_heads:], "tp", partner)

    own_inner = own_heads * HD
    fresh_rows = main[rows : rows + sequences]
    new_position = jnp.full((1,), groups * span_len, jnp.int32)
    new_key = fresh_rows[:, :own_inner].reshape(sequences, 1, own_heads, HD)
    new_key = (rotate(new_key, new_position) * key_scale).astype(jnp.bfloat16)[:, 0]
    new_value = fresh_rows[:, inner : inner + own_inner].reshape(sequences, own_heads, HD)
    new_value = new_value.astype(jnp.bfloat16)
    new_query = query[:sequences].reshape(sequences, 1, own_heads, HD)
    new_query = rotate(new_query, new_position).astype(jnp.bfloat16)[:, 0]
    query_entries = new_query.astype(jnp.float32)
    own_term = jnp.sum(
        query_entries * new_key.astype(jnp.float32), axis=-1, keepdims=True
    ) * new_value.astype(jnp.float32)
    partial_read = jnp.sum(state * query_entries[..., None], axis=2) * jnp.exp(log_decay)[None, :, None]

    pairs_y = {
        d: [(4 * y + x, 4 * ((y + d) % side) + x) for y in range(side) for x in range(side)]
        for d in range(1, side)
    }
    pairs_x = {
        d: [(4 * y + x, 4 * y + (x + d) % side) for y in range(side) for x in range(side)]
        for d in range(1, side)
    }
    own_y = own_index // side
    own_x = own_index % side
    outer = sequences * own_heads
    flat = state.reshape(outer, side, HD // side, HD)
    flat = jnp.moveaxis(flat, 1, 0)
    read_row = jnp.broadcast_to(partial_read.reshape(1, outer, 1, HD), (side, outer, 1, HD))
    flat = exchange_sum(jnp.concatenate([flat, read_row], axis=2), pairs_y, own_y, side)
    read_row = flat[:, HD // side :]
    flat = flat[:, : HD // side].reshape(outer, side, HD // side // side, HD)
    flat = jnp.moveaxis(flat, 1, 0)
    read_row = jnp.broadcast_to(read_row[None], (side, outer, 1, HD))
    flat = exchange_sum(jnp.concatenate([flat, read_row], axis=2), pairs_x, own_x, side)
    keep = HD // groups
    state_rows = flat[:, :keep].reshape(sequences, own_heads, keep, HD)
    summed = flat[:, keep].reshape(sequences, own_heads, HD)
    normed = group_norm(summed + own_term)
    return (
        state_rows.astype(jnp.bfloat16),
        normed.reshape(sequences, own_inner).astype(jnp.bfloat16),
    )


def solution(mesh):
    return jax.shard_map(
        body,
        mesh=mesh,
        in_specs=(
            P(None, "sp", "tp"),
            P(None, None, "tp"),
            P(None, "tp"),
            P(None, "tp"),
            P(None, "tp"),
            P("tp"),
        ),
        out_specs=(P(None, "tp", "sp", None), P(None, "tp")),
        check_vma=False,
    )
```

```python
import jax
import jax.numpy as jnp
from jax import lax
from jax.sharding import PartitionSpec as P

HD = 64


def rotate(values, positions):
    half_dim = values.shape[-1] // 2
    inverse = 10000.0 ** (-jnp.arange(half_dim, dtype=jnp.float32) / half_dim)
    angles = positions.astype(jnp.float32)[:, None, None] * inverse[None, None, :]
    cosine = jnp.cos(angles)
    sine_part = jnp.sin(angles)
    first = values[..., :half_dim]
    second = values[..., half_dim:]
    return jnp.concatenate(
        [first * cosine - second * sine_part, first * sine_part + second * cosine], axis=-1
    )


def group_norm(output):
    centered = output - jnp.mean(output, axis=-1, keepdims=True)
    return centered * lax.rsqrt(jnp.mean(centered * centered, axis=-1, keepdims=True) + 1e-05)


def body(tokens, new_token, query_weight, key_weight, value_weight, log_decay):
    sequences, span_len, width = tokens.shape
    own_heads = log_decay.shape[0]
    groups = lax.axis_size("sp")
    planes = lax.axis_size("tp") // 2
    own_index = lax.axis_index("sp")
    tp_index = lax.axis_index("tp")
    plane = tp_index // 2
    core = tp_index % 2
    key_scale = HD ** (-0.5)
    half = span_len // 2
    rows = sequences * half
    extra = 16

    partner = [(i, i ^ 1) for i in range(2 * planes)]

    def ring(sign):
        return [
            (2 * z + c, 2 * ((z + (sign if c == 0 else -sign)) % planes) + c)
            for z in range(planes)
            for c in range(2)
        ]

    near_ring = ring(1)
    far_ring = ring(-1)

    fresh = jnp.concatenate(
        [new_token[:, 0], jnp.zeros((extra - sequences, width), new_token.dtype)], axis=0
    )

    def part(which):
        piece = lax.dynamic_slice_in_dim(tokens, which * half, half, 1).reshape(rows, width)
        return jnp.concatenate([piece, fresh], axis=0)

    mine = part(core)
    theirs = lax.ppermute(part(1 - core), "tp", partner)
    chunk = jnp.where(
        core == 0,
        jnp.concatenate([mine, theirs], axis=1),
        jnp.concatenate([theirs, mine], axis=1),
    )

    key_other = lax.ppermute(key_weight, "tp", partner)
    value_other = lax.ppermute(value_weight, "tp", partner)
    decay_other = lax.ppermute(log_decay, "tp", partner)
    row_weights = jnp.concatenate([key_weight, key_other, value_weight, value_other], axis=1)
    row_weights = row_weights.reshape(planes, 2 * width, row_weights.shape[1])
    query_rows = query_weight.reshape(planes, 2 * width, query_weight.shape[1])
    toward = 1 - 2 * core

    def project(both, offset):
        at = (plane + offset * toward) % planes
        main = jnp.dot(
            both,
            lax.dynamic_index_in_dim(row_weights, at, 0, keepdims=False),
            preferred_element_type=jnp.float32,
        )
        query = jnp.dot(
            both[rows:],
            lax.dynamic_index_in_dim(query_rows, at, 0, keepdims=False),
            preferred_element_type=jnp.float32,
        )
        return main, query

    main, query = project(chunk, 0)
    near = far = chunk
    reach = planes // 2
    for step in range(1, reach + 1):
        near = lax.ppermute(near, "tp", near_ring)
        pieces = [(near, -step)]
        if step < reach:
            far = lax.ppermute(far, "tp", far_ring)
            pieces.append((far, step))
        for both, offset in pieces:
            more, more_query = project(both, offset)
            main = main + more
            query = query + more_query

    heads = 2 * own_heads
    inner = heads * HD
    decay = jnp.concatenate([log_decay, decay_other])
    key_rows = main[:rows, :inner].reshape(sequences, half, heads, HD)
    value_rows = main[:rows, inner:].reshape(sequences, half, heads, HD).astype(jnp.bfloat16)
    local = core * half + jnp.arange(half, dtype=jnp.int32)
    key_rows = (rotate(key_rows, own_index * span_len + local) * key_scale).astype(jnp.bfloat16)
    to_end = (span_len - 1 - local).astype(jnp.float32)
    decay_rows = jnp.exp(to_end[:, None] * decay[None, :])
    weighted = (key_rows.astype(jnp.float32) * decay_rows[None, :, :, None]).astype(jnp.bfloat16)
    span_state = jnp.einsum(
        "sthk,sthv->shkv", weighted, value_rows, preferred_element_type=jnp.float32
    )
    carried = jnp.exp(decay * (span_len * (groups - 1 - own_index)).astype(jnp.float32))
    scaled = span_state * carried[None, :, None, None]
    state = scaled[:, :own_heads] + lax.ppermute(scaled[:, own_heads:], "tp", partner)

    own_inner = own_heads * HD
    fresh_rows = main[rows : rows + sequences]
    new_position = jnp.full((1,), groups * span_len, jnp.int32)
    new_key = fresh_rows[:, :own_inner].reshape(sequences, 1, own_heads, HD)
    new_key = (rotate(new_key, new_position) * key_scale).astype(jnp.bfloat16)[:, 0]
    new_value = fresh_rows[:, inner : inner + own_inner].reshape(sequences, own_heads, HD)
    new_value = new_value.astype(jnp.bfloat16)
    new_query = query[:sequences].reshape(sequences, 1, own_heads, HD)
    new_query = rotate(new_query, new_position).astype(jnp.bfloat16)[:, 0]
    query_entries = new_query.astype(jnp.float32)
    own_term = jnp.sum(
        query_entries * new_key.astype(jnp.float32), axis=-1, keepdims=True
    ) * new_value.astype(jnp.float32)
    partial_read = jnp.sum(state * query_entries[..., None], axis=2) * jnp.exp(log_decay)[None, :, None]

    outer = sequences * own_heads
    keep = HD // groups
    pieces = jnp.moveaxis(state.reshape(outer, groups, keep * HD), 1, 0).reshape(groups, -1)
    reads = jnp.broadcast_to(partial_read.reshape(1, outer * HD), (groups, outer * HD))
    packed = jnp.concatenate([pieces, reads], axis=1)
    packed = packed.reshape(groups, packed.shape[1] // 128, 128)
    arrived = lax.all_to_all(packed, "sp", split_axis=0, concat_axis=0, tiled=True)
    arrived = jnp.sum(arrived, axis=0).reshape(-1)
    count = outer * keep * HD
    state_rows = arrived[:count].reshape(sequences, own_heads, keep, HD)
    summed = arrived[count:].reshape(sequences, own_heads, HD)
    normed = group_norm(summed + own_term)
    return (
        state_rows.astype(jnp.bfloat16),
        normed.reshape(sequences, own_inner).astype(jnp.bfloat16),
    )


def solution(mesh):
    return jax.shard_map(
        body,
        mesh=mesh,
        in_specs=(
            P(None, "sp", "tp"),
            P(None, None, "tp"),
            P(None, "tp"),
            P(None, "tp"),
            P(None, "tp"),
            P("tp"),
        ),
        out_specs=(P(None, "tp", "sp", None), P(None, "tp")),
        check_vma=False,
    )
```

```python
import jax
import jax.numpy as jnp
from jax import lax
from jax.experimental import pallas as pl
from jax.experimental.pallas import tpu as pltpu
from jax.sharding import PartitionSpec as P

HD = 64
EPS = 1e-05
STEP = 8


def swap_halves(values):
    lanes = values.shape[-1]
    lane = lax.broadcasted_iota(jnp.int32, values.shape, len(values.shape) - 1)
    quarter = HD // 2
    back = pltpu.roll(values, lanes - quarter, len(values.shape) - 1)
    ahead = pltpu.roll(values, quarter, len(values.shape) - 1)
    return jnp.where(lane % HD < quarter, back, ahead)


def state_kernel(
    x_ref, kw_ref, vw_ref, cos_ref, sin_ref, decay_ref, carried_ref, query_ref, one_ref, out_ref, acc
):
    prompt = pl.program_id(0)
    step = pl.program_id(1)
    blocks = [x_ref[i, 0] for i in range(STEP)]
    both = jnp.concatenate(blocks, axis=1)
    width = both.shape[1]
    at = pl.ds(pl.multiple_of(step * width, width), width)
    weights = jnp.concatenate([kw_ref[at, :], vw_ref[at, :]], axis=1)
    part = jnp.dot(both, weights, preferred_element_type=jnp.float32)

    @pl.when(step == 0)
    def _():
        acc[...] = part

    @pl.when(step > 0)
    def _():
        acc[...] += part

    @pl.when(step == pl.num_programs(1) - 1)
    def _():
        inner = kw_ref.shape[1]
        total = acc[...]
        keys = total[:, :inner]
        values = total[:, inner:].astype(jnp.bfloat16)
        keys = (keys * cos_ref[...] + swap_halves(keys) * sin_ref[...]).astype(jnp.bfloat16)
        weighted = (keys.astype(jnp.float32) * decay_ref[...]).astype(jnp.bfloat16)
        full = lax.dot_general(
            weighted, values, (((0,), (0,)), ((), ())), preferred_element_type=jnp.float32
        )
        lane = lax.broadcasted_iota(jnp.int32, (HD, inner), 1)
        state = jnp.where(lane < HD, full[:HD], full[HD:]) * carried_ref[...]
        read = jnp.sum(state * query_ref[0], axis=0, keepdims=True) * one_ref[...]
        groups = out_ref.shape[0]
        keep = HD // groups
        count = out_ref.shape[1] // (keep + 1)
        for s in range(count):

            @pl.when(prompt == s)
            def _():
                for g in range(groups):
                    out_ref[g, s * keep : (s + 1) * keep, :] = state[g * keep : (g + 1) * keep]
                    out_ref[g, count * keep + s : count * keep + s + 1, :] = read


def span_states(gathered, key_weight, value_weight, cosine, sine, decay, carried, query, one, groups):
    devices, prompts, span_len, width = gathered.shape
    inner = key_weight.shape[1]
    keep = HD // groups
    out_rows = prompts * (keep + 1)
    whole = pl.BlockSpec(memory_space=pltpu.VMEM)
    return pl.pallas_call(
        state_kernel,
        grid=(prompts, devices // STEP),
        in_specs=[
            pl.BlockSpec((STEP, 1, span_len, width), lambda s, k: (k, s, 0, 0)),
            whole,
            whole,
            whole,
            whole,
            whole,
            whole,
            pl.BlockSpec((1, HD, inner), lambda s, k: (s, 0, 0)),
            whole,
        ],
        out_specs=pl.BlockSpec((groups, out_rows, inner), lambda s, k: (0, 0, 0)),
        out_shape=jax.ShapeDtypeStruct((groups, out_rows, inner), jnp.float32),
        scratch_shapes=[pltpu.VMEM((span_len, 2 * inner), jnp.float32)],
        compiler_params=pltpu.CompilerParams(
            dimension_semantics=("arbitrary", "arbitrary"), vmem_limit_bytes=53 * 1024 * 1024
        ),
        name="span_states",
    )(gathered, key_weight, value_weight, cosine, sine, decay, carried, query, one)


def finish_kernel(arrived_ref, own_ref, state_ref, read_ref):
    total = jnp.sum(arrived_ref[...], axis=0)
    prompts, heads, keep, _ = state_ref.shape
    for s in range(prompts):
        for h in range(heads):
            state_ref[s, h] = total[s * keep : (s + 1) * keep, h * HD : (h + 1) * HD].astype(
                jnp.bfloat16
            )
    raw = total[prompts * keep :] + own_ref[...]
    lane = lax.broadcasted_iota(jnp.int32, raw.shape, 1)

    def per_head(values):
        result = jnp.zeros_like(values)
        for h in range(heads):
            here = lane // HD == h
            mean = jnp.sum(jnp.where(here, values, 0.0), axis=1, keepdims=True) / HD
            result = jnp.where(here, mean, result)
        return result

    centered = raw - per_head(raw)
    spread = per_head(centered * centered)
    read_ref[...] = (centered * lax.rsqrt(spread + EPS)).astype(jnp.bfloat16)


def finish(arrived, own_term, heads, keep):
    prompts, inner = own_term.shape
    whole = pl.BlockSpec(memory_space=pltpu.VMEM)
    return pl.pallas_call(
        finish_kernel,
        in_specs=[whole, whole],
        out_specs=[whole, whole],
        out_shape=[
            jax.ShapeDtypeStruct((prompts, heads, keep, HD), jnp.bfloat16),
            jax.ShapeDtypeStruct((prompts, inner), jnp.bfloat16),
        ],
        compiler_params=pltpu.CompilerParams(vmem_limit_bytes=4 * 1024 * 1024),
        name="finish",
    )(arrived, own_term)


def angles_at(positions, heads):
    half_dim = HD // 2
    inverse = 10000.0 ** (-jnp.arange(half_dim, dtype=jnp.float32) / half_dim)
    angles = positions.astype(jnp.float32)[:, None] * inverse[None, :]
    cosine = jnp.cos(angles)
    sine = jnp.sin(angles)
    cosine = jnp.tile(jnp.concatenate([cosine, cosine], axis=1), (1, heads))
    sine = jnp.tile(jnp.concatenate([-sine, sine], axis=1), (1, heads))
    return cosine, sine


def rotate(values, cosine, sine):
    half_dim = HD // 2
    swapped = values.reshape(values.shape[0], -1, 2, half_dim)[:, :, ::-1].reshape(values.shape)
    return values * cosine + swapped * sine


def body(tokens, new_token, query_weight, key_weight, value_weight, log_decay):
    prompts, span_len, width = tokens.shape
    heads = log_decay.shape[0]
    inner = heads * HD
    groups = lax.axis_size("sp")
    own_index = lax.axis_index("sp")
    key_scale = HD ** (-0.5)

    gathered = lax.all_gather(tokens, "tp", axis=0, tiled=False)
    fresh = lax.all_gather(new_token[:, 0], "tp", axis=0, tiled=False)

    local = jnp.arange(span_len, dtype=jnp.int32)
    cosine, sine = angles_at(own_index * span_len + local, heads)
    to_end = (span_len - 1 - local).astype(jnp.float32)
    lane_decay = jnp.repeat(log_decay, HD)
    decay_rows = jnp.exp(to_end[:, None] * lane_decay[None, :])
    distance = (span_len * (groups - 1 - own_index)).astype(jnp.float32)
    carried = jnp.exp(lane_decay * distance)[None, :]
    one = jnp.exp(lane_decay)[None, :]

    all_weights = jnp.concatenate([key_weight, value_weight, query_weight], axis=1)
    fresh = jnp.moveaxis(fresh, 0, 1).reshape(prompts, -1)
    new_total = jnp.dot(fresh, all_weights, preferred_element_type=jnp.float32)
    new_cosine, new_sine = angles_at(jnp.full((1,), groups * span_len, jnp.int32), heads)
    new_key = (rotate(new_total[:, :inner], new_cosine, new_sine) * key_scale).astype(jnp.bfloat16)
    new_value = new_total[:, inner : 2 * inner].astype(jnp.bfloat16).astype(jnp.float32)
    new_query = rotate(new_total[:, 2 * inner :], new_cosine, new_sine).astype(jnp.bfloat16)
    new_query = new_query.astype(jnp.float32)
    score = jnp.sum(
        (new_query * new_key.astype(jnp.float32)).reshape(prompts, heads, HD), axis=-1, keepdims=True
    )
    own_term = (score * new_value.reshape(prompts, heads, HD)).reshape(prompts, inner)
    query = jnp.swapaxes(new_query.reshape(prompts, heads, HD), 1, 2)
    query = jnp.repeat(query, HD, axis=2)

    messages = span_states(
        gathered,
        key_weight,
        value_weight,
        cosine * key_scale,
        sine * key_scale,
        decay_rows,
        carried,
        query,
        one,
        groups,
    )
    arrived = lax.all_to_all(messages, "sp", split_axis=0, concat_axis=0, tiled=True)
    return tuple(finish(arrived, own_term, heads, HD // groups))


def solution(mesh):
    return jax.shard_map(
        body,
        mesh=mesh,
        in_specs=(
            P(None, "sp", "tp"),
            P(None, None, "tp"),
            P(None, "tp"),
            P(None, "tp"),
            P(None, "tp"),
            P("tp"),
        ),
        out_specs=(P(None, "tp", "sp", None), P(None, "tp")),
        check_vma=False,
    )
```

```python
import jax
import jax.numpy as jnp
from jax import lax
from jax.experimental import pallas as pl
from jax.experimental.pallas import tpu as pltpu
from jax.sharding import PartitionSpec as P

HD = 64
EPS = 1e-05
STEP = 16


def swap_halves(values):
    lanes = values.shape[-1]
    lane = lax.broadcasted_iota(jnp.int32, values.shape, len(values.shape) - 1)
    quarter = HD // 2
    back = pltpu.roll(values, lanes - quarter, len(values.shape) - 1)
    ahead = pltpu.roll(values, quarter, len(values.shape) - 1)
    return jnp.where(lane % HD < quarter, back, ahead)


def state_kernel(
    x_ref,
    kw_ref,
    vw_ref,
    cos_ref,
    sin_ref,
    decay_ref,
    carried_ref,
    query_ref,
    one_ref,
    out_ref,
    held,
    arrived,
):
    devices, prompts, _, width = x_ref.shape
    inner = kw_ref.shape[1]
    groups = out_ref.shape[0]
    keep = HD // groups
    pieces = devices // STEP
    copies = [
        pltpu.make_async_copy(
            x_ref.at[pl.ds(k * STEP, STEP), s],
            held.at[s, pl.ds(k * STEP, STEP)],
            arrived.at[s * pieces + k],
        )
        for s in range(prompts)
        for k in range(pieces)
    ]
    for copy in copies:
        copy.start()
    lane = lax.broadcasted_iota(jnp.int32, (HD, inner), 1)
    for s in range(prompts):
        total = None
        for k in range(pieces):
            copies[s * pieces + k].wait()
            both = jnp.concatenate([held[s, k * STEP + i] for i in range(STEP)], axis=1)
            at = pl.ds(k * STEP * width, STEP * width)
            weights = jnp.concatenate([kw_ref[at, :], vw_ref[at, :]], axis=1)
            part = jnp.dot(both, weights, preferred_element_type=jnp.float32)
            total = part if total is None else total + part
        keys = total[:, :inner]
        values = total[:, inner:].astype(jnp.bfloat16)
        keys = (keys * cos_ref[...] + swap_halves(keys) * sin_ref[...]).astype(jnp.bfloat16)
        weighted = (keys.astype(jnp.float32) * decay_ref[...]).astype(jnp.bfloat16)
        full = lax.dot_general(
            weighted, values, (((0,), (0,)), ((), ())), preferred_element_type=jnp.float32
        )
        state = jnp.where(lane < HD, full[:HD], full[HD:]) * carried_ref[...]
        read = jnp.sum(state * query_ref[s], axis=0, keepdims=True) * one_ref[...]
        for g in range(groups):
            out_ref[g, s * keep : (s + 1) * keep, :] = state[g * keep : (g + 1) * keep]
            out_ref[g, prompts * keep + s : prompts * keep + s + 1, :] = read


def span_states(gathered, key_weight, value_weight, cosine, sine, decay, carried, query, one, groups):
    devices, prompts, span_len, width = gathered.shape
    inner = key_weight.shape[1]
    keep = HD // groups
    whole = pl.BlockSpec(memory_space=pltpu.VMEM)
    return pl.pallas_call(
        state_kernel,
        in_specs=[pl.BlockSpec(memory_space=pltpu.HBM)] + [whole] * 8,
        out_specs=whole,
        out_shape=jax.ShapeDtypeStruct((groups, prompts * (keep + 1), inner), jnp.float32),
        scratch_shapes=[
            pltpu.VMEM((prompts, devices, span_len, width), gathered.dtype),
            pltpu.SemaphoreType.DMA((prompts * (devices // STEP),)),
        ],
        compiler_params=pltpu.CompilerParams(vmem_limit_bytes=53 * 1024 * 1024),
        name="span_states",
    )(gathered, key_weight, value_weight, cosine, sine, decay, carried, query, one)


def finish_kernel(arrived_ref, own_ref, state_ref, read_ref):
    total = jnp.sum(arrived_ref[...], axis=0)
    prompts, heads, keep, _ = state_ref.shape
    for s in range(prompts):
        for h in range(heads):
            state_ref[s, h] = total[s * keep : (s + 1) * keep, h * HD : (h + 1) * HD].astype(
                jnp.bfloat16
            )
    raw = total[prompts * keep :] + own_ref[...]
    lane = lax.broadcasted_iota(jnp.int32, raw.shape, 1)

    def per_head(values):
        result = jnp.zeros_like(values)
        for h in range(heads):
            here = lane // HD == h
            mean = jnp.sum(jnp.where(here, values, 0.0), axis=1, keepdims=True) / HD
            result = jnp.where(here, mean, result)
        return result

    centered = raw - per_head(raw)
    spread = per_head(centered * centered)
    read_ref[...] = (centered * lax.rsqrt(spread + EPS)).astype(jnp.bfloat16)


def finish(arrived, own_term, heads, keep):
    prompts, inner = own_term.shape
    whole = pl.BlockSpec(memory_space=pltpu.VMEM)
    return pl.pallas_call(
        finish_kernel,
        in_specs=[whole, whole],
        out_specs=[whole, whole],
        out_shape=[
            jax.ShapeDtypeStruct((prompts, heads, keep, HD), jnp.bfloat16),
            jax.ShapeDtypeStruct((prompts, inner), jnp.bfloat16),
        ],
        compiler_params=pltpu.CompilerParams(vmem_limit_bytes=4 * 1024 * 1024),
        name="finish",
    )(arrived, own_term)


def angles_at(positions, heads):
    half_dim = HD // 2
    inverse = 10000.0 ** (-jnp.arange(half_dim, dtype=jnp.float32) / half_dim)
    angles = positions.astype(jnp.float32)[:, None] * inverse[None, :]
    cosine = jnp.cos(angles)
    sine = jnp.sin(angles)
    cosine = jnp.tile(jnp.concatenate([cosine, cosine], axis=1), (1, heads))
    sine = jnp.tile(jnp.concatenate([-sine, sine], axis=1), (1, heads))
    return cosine, sine


def rotate(values, cosine, sine):
    half_dim = HD // 2
    swapped = values.reshape(values.shape[0], -1, 2, half_dim)[:, :, ::-1].reshape(values.shape)
    return values * cosine + swapped * sine


def body(tokens, new_token, query_weight, key_weight, value_weight, log_decay):
    prompts, span_len, width = tokens.shape
    heads = log_decay.shape[0]
    inner = heads * HD
    groups = lax.axis_size("sp")
    own_index = lax.axis_index("sp")
    key_scale = HD ** (-0.5)

    gathered = lax.all_gather(tokens, "tp", axis=0, tiled=False)
    fresh = lax.all_gather(new_token[:, 0], "tp", axis=0, tiled=False)

    local = jnp.arange(span_len, dtype=jnp.int32)
    cosine, sine = angles_at(own_index * span_len + local, heads)
    to_end = (span_len - 1 - local).astype(jnp.float32)
    lane_decay = jnp.repeat(log_decay, HD)
    decay_rows = jnp.exp(to_end[:, None] * lane_decay[None, :])
    distance = (span_len * (groups - 1 - own_index)).astype(jnp.float32)
    carried = jnp.exp(lane_decay * distance)[None, :]
    one = jnp.exp(lane_decay)[None, :]

    all_weights = jnp.concatenate([key_weight, value_weight, query_weight], axis=1)
    fresh = jnp.moveaxis(fresh, 0, 1).reshape(prompts, -1)
    new_total = jnp.dot(fresh, all_weights, preferred_element_type=jnp.float32)
    new_cosine, new_sine = angles_at(jnp.full((1,), groups * span_len, jnp.int32), heads)
    new_key = (rotate(new_total[:, :inner], new_cosine, new_sine) * key_scale).astype(jnp.bfloat16)
    new_value = new_total[:, inner : 2 * inner].astype(jnp.bfloat16).astype(jnp.float32)
    new_query = rotate(new_total[:, 2 * inner :], new_cosine, new_sine).astype(jnp.bfloat16)
    new_query = new_query.astype(jnp.float32)
    score = jnp.sum(
        (new_query * new_key.astype(jnp.float32)).reshape(prompts, heads, HD), axis=-1, keepdims=True
    )
    own_term = (score * new_value.reshape(prompts, heads, HD)).reshape(prompts, inner)
    query = jnp.swapaxes(new_query.reshape(prompts, heads, HD), 1, 2)
    query = jnp.repeat(query, HD, axis=2)

    messages = span_states(
        gathered,
        key_weight,
        value_weight,
        cosine * key_scale,
        sine * key_scale,
        decay_rows,
        carried,
        query,
        one,
        groups,
    )
    arrived = lax.all_to_all(messages, "sp", split_axis=0, concat_axis=0, tiled=True)
    return tuple(finish(arrived, own_term, heads, HD // groups))


def solution(mesh):
    return jax.shard_map(
        body,
        mesh=mesh,
        in_specs=(
            P(None, "sp", "tp"),
            P(None, None, "tp"),
            P(None, "tp"),
            P(None, "tp"),
            P(None, "tp"),
            P("tp"),
        ),
        out_specs=(P(None, "tp", "sp", None), P(None, "tp")),
        check_vma=False,
    )
```

```python
import jax
import jax.numpy as jnp
from jax import lax
from jax.experimental import pallas as pl
from jax.experimental.pallas import tpu as pltpu
from jax.sharding import PartitionSpec as P

HD = 64
EPS = 1e-05
EXTRA = 16


def swap_halves(values):
    lanes = values.shape[-1]
    lane = lax.broadcasted_iota(jnp.int32, values.shape, len(values.shape) - 1)
    quarter = HD // 2
    back = pltpu.roll(values, lanes - quarter, len(values.shape) - 1)
    ahead = pltpu.roll(values, quarter, len(values.shape) - 1)
    return jnp.where(lane % HD < quarter, back, ahead)


def state_kernel(
    total_ref,
    arrived_ref,
    query_ref,
    last_a_ref,
    last_b_ref,
    weight_ref,
    query_weight_ref,
    cos_ref,
    sin_ref,
    decay_ref,
    carried_ref,
    one_ref,
    new_cos_ref,
    new_sin_ref,
    out_ref,
    own_ref,
):
    span_len, inner = decay_ref.shape
    rows = last_a_ref.shape[0] - EXTRA
    prompts = rows // span_len
    groups = out_ref.shape[0]
    keep = HD // groups
    key_scale = HD ** (-0.5)
    lane = lax.broadcasted_iota(jnp.int32, (HD, inner), 1)

    def projected(start, count):
        at = pl.ds(start, count)
        last = jnp.concatenate([last_a_ref[at, :], last_b_ref[at, :]], axis=1)
        part = jnp.dot(last, weight_ref[...], preferred_element_type=jnp.float32)
        return total_ref[at, :] + arrived_ref[at, :] + part

    fresh = projected(rows, EXTRA)
    last = jnp.concatenate([last_a_ref[rows:, :], last_b_ref[rows:, :]], axis=1)
    query = query_ref[...] + arrived_ref[rows + EXTRA :, :inner]
    query += jnp.dot(last, query_weight_ref[...], preferred_element_type=jnp.float32)
    query = query * new_cos_ref[...] + swap_halves(query) * new_sin_ref[...]
    query = query.astype(jnp.bfloat16).astype(jnp.float32)
    new_key = fresh[:, :inner]
    new_key = (new_key * new_cos_ref[...] + swap_halves(new_key) * new_sin_ref[...]) * key_scale
    new_key = new_key.astype(jnp.bfloat16).astype(jnp.float32)
    new_value = fresh[:, inner:].astype(jnp.bfloat16).astype(jnp.float32)
    products = query * new_key
    new_lane = lax.broadcasted_iota(jnp.int32, products.shape, 1)
    score = jnp.zeros_like(products)
    for h in range(inner // HD):
        here = new_lane // HD == h
        score = jnp.where(
            here, jnp.sum(jnp.where(here, products, 0.0), axis=1, keepdims=True), score
        )
    own_ref[...] = score * new_value
    columns = jnp.transpose(query)

    for s in range(prompts):
        total = projected(s * span_len, span_len)
        keys = total[:, :inner]
        values = total[:, inner:].astype(jnp.bfloat16)
        keys = (keys * cos_ref[...] + swap_halves(keys) * sin_ref[...]).astype(jnp.bfloat16)
        weighted = (keys.astype(jnp.float32) * decay_ref[...]).astype(jnp.bfloat16)
        full = lax.dot_general(
            weighted, values, (((0,), (0,)), ((), ())), preferred_element_type=jnp.float32
        )
        state = jnp.where(lane < HD, full[:HD], full[HD:]) * carried_ref[...]
        entries = jnp.where(lane < HD, columns[:HD, s : s + 1], columns[HD:, s : s + 1])
        read = jnp.sum(state * entries, axis=0, keepdims=True) * one_ref[...]
        for g in range(groups):
            out_ref[g, s * keep : (s + 1) * keep, :] = state[g * keep : (g + 1) * keep]
            out_ref[g, prompts * keep + s : prompts * keep + s + 1, :] = read


def span_states(prompts, groups, decay, *operands):
    inner = decay.shape[1]
    keep = HD // groups
    whole = pl.BlockSpec(memory_space=pltpu.VMEM)
    return pl.pallas_call(
        state_kernel,
        in_specs=[whole] * len(operands),
        out_specs=[whole, whole],
        out_shape=[
            jax.ShapeDtypeStruct((groups, prompts * (keep + 1), inner), jnp.float32),
            jax.ShapeDtypeStruct((EXTRA, inner), jnp.float32),
        ],
        compiler_params=pltpu.CompilerParams(vmem_limit_bytes=24 * 1024 * 1024),
        name="span_states",
    )(*operands)


def finish_kernel(arrived_ref, own_ref, state_ref, read_ref):
    total = jnp.sum(arrived_ref[...], axis=0)
    prompts, heads, keep, _ = state_ref.shape
    for s in range(prompts):
        for h in range(heads):
            state_ref[s, h] = total[s * keep : (s + 1) * keep, h * HD : (h + 1) * HD].astype(
                jnp.bfloat16
            )
    raw = total[prompts * keep :] + own_ref[:prompts, :]
    lane = lax.broadcasted_iota(jnp.int32, raw.shape, 1)

    def per_head(values):
        result = jnp.zeros_like(values)
        for h in range(heads):
            here = lane // HD == h
            mean = jnp.sum(jnp.where(here, values, 0.0), axis=1, keepdims=True) / HD
            result = jnp.where(here, mean, result)
        return result

    centered = raw - per_head(raw)
    spread = per_head(centered * centered)
    read_ref[...] = (centered * lax.rsqrt(spread + EPS)).astype(jnp.bfloat16)


def finish(arrived, own_term, prompts, heads, keep):
    inner = own_term.shape[1]
    whole = pl.BlockSpec(memory_space=pltpu.VMEM)
    return pl.pallas_call(
        finish_kernel,
        in_specs=[whole, whole],
        out_specs=[whole, whole],
        out_shape=[
            jax.ShapeDtypeStruct((prompts, heads, keep, HD), jnp.bfloat16),
            jax.ShapeDtypeStruct((prompts, inner), jnp.bfloat16),
        ],
        compiler_params=pltpu.CompilerParams(vmem_limit_bytes=4 * 1024 * 1024),
        name="finish",
    )(arrived, own_term)


def angles_at(positions, heads):
    half_dim = HD // 2
    inverse = 10000.0 ** (-jnp.arange(half_dim, dtype=jnp.float32) / half_dim)
    angles = positions.astype(jnp.float32)[:, None] * inverse[None, :]
    cosine = jnp.cos(angles)
    sine = jnp.sin(angles)
    cosine = jnp.tile(jnp.concatenate([cosine, cosine], axis=1), (1, heads))
    sine = jnp.tile(jnp.concatenate([-sine, sine], axis=1), (1, heads))
    return cosine, sine


def body(tokens, new_token, query_weight, key_weight, value_weight, log_decay):
    prompts, span_len, width = tokens.shape
    heads = log_decay.shape[0]
    inner = heads * HD
    groups = lax.axis_size("sp")
    own_index = lax.axis_index("sp")
    tp_index = lax.axis_index("tp")
    planes = lax.axis_size("tp") // 2
    plane = tp_index // 2
    core = tp_index % 2
    toward = 1 - 2 * core
    rows = prompts * span_len
    key_scale = HD ** (-0.5)

    partner = [(i, i ^ 1) for i in range(2 * planes)]
    onward = [
        (2 * z + c, 2 * ((z + (1 if c == 0 else -1)) % planes) + c)
        for z in range(planes)
        for c in range(2)
    ]

    fresh = jnp.concatenate(
        [new_token[:, 0], jnp.zeros((EXTRA - prompts, width), new_token.dtype)], axis=0
    )
    chain_a = jnp.concatenate([tokens.reshape(rows, width), fresh], axis=0)
    chain_b = lax.ppermute(chain_a, "tp", partner)

    def other(weights):
        return lax.ppermute(weights, "tp", partner)

    main_weights = jnp.concatenate([key_weight, value_weight], axis=1)
    all_weights = jnp.concatenate(
        [main_weights, other(key_weight), other(value_weight)], axis=1
    ).reshape(2 * planes, width, 4 * inner)
    main_weights = main_weights.reshape(2 * planes, width, 2 * inner)
    own_query = query_weight.reshape(2 * planes, width, inner)
    all_query = jnp.concatenate([query_weight, other(query_weight)], axis=1)
    all_query = all_query.reshape(2 * planes, width, 2 * inner)

    def places(offset):
        at = (plane - offset * toward) % planes
        return 2 * at + core, 2 * at + 1 - core

    def block(weights, at):
        return lax.dynamic_index_in_dim(weights, at, 0, keepdims=False)

    def project(a, b, offset, weights, queries):
        at_a, at_b = places(offset)
        main = jnp.dot(a, block(weights, at_a), preferred_element_type=jnp.float32)
        main = main + jnp.dot(b, block(weights, at_b), preferred_element_type=jnp.float32)
        query = jnp.dot(a[rows:], block(queries, at_a), preferred_element_type=jnp.float32)
        query = query + jnp.dot(b[rows:], block(queries, at_b), preferred_element_type=jnp.float32)
        return main, query

    own_main, own_query_rows = project(chain_a, chain_b, 0, main_weights, own_query)
    reach = planes // 2
    main = query = None
    for step in range(1, reach):
        chain_a = lax.ppermute(chain_a, "tp", onward)
        chain_b = lax.ppermute(chain_b, "tp", onward)
        more, more_query = project(chain_a, chain_b, step, all_weights, all_query)
        main = more if main is None else main + more
        query = more_query if query is None else query + more_query
        main, query = lax.optimization_barrier((main, query))
    last_a = lax.ppermute(chain_a, "tp", onward)
    last_b = lax.ppermute(chain_b, "tp", onward)

    outgoing = jnp.concatenate(
        [main[:, 2 * inner :], jnp.concatenate([query[:, inner:]] * 2, axis=1)], axis=0
    )
    arrived = lax.ppermute(outgoing, "tp", partner)
    own_main = own_main + main[:, : 2 * inner]
    own_query_rows = own_query_rows + query[:, :inner]
    at_a, at_b = places(reach)
    last_weights = jnp.concatenate([block(main_weights, at_a), block(main_weights, at_b)], axis=0)
    last_query = jnp.concatenate([block(own_query, at_a), block(own_query, at_b)], axis=0)

    local = jnp.arange(span_len, dtype=jnp.int32)
    cosine, sine = angles_at(own_index * span_len + local, heads)
    to_end = (span_len - 1 - local).astype(jnp.float32)
    lane_decay = jnp.repeat(log_decay, HD)
    decay_rows = jnp.exp(to_end[:, None] * lane_decay[None, :])
    distance = (span_len * (groups - 1 - own_index)).astype(jnp.float32)
    carried = jnp.exp(lane_decay * distance)[None, :]
    one = jnp.exp(lane_decay)[None, :]
    new_cosine, new_sine = angles_at(jnp.full((1,), groups * span_len, jnp.int32), heads)

    messages, own_term = span_states(
        prompts,
        groups,
        decay_rows,
        own_main,
        arrived,
        own_query_rows,
        last_a,
        last_b,
        last_weights,
        last_query,
        cosine * key_scale,
        sine * key_scale,
        decay_rows,
        carried,
        one,
        new_cosine,
        new_sine,
    )
    arrived = lax.all_to_all(messages, "sp", split_axis=0, concat_axis=0, tiled=True)
    return tuple(finish(arrived, own_term, prompts, heads, HD // groups))


def solution(mesh):
    return jax.shard_map(
        body,
        mesh=mesh,
        in_specs=(
            P(None, "sp", "tp"),
            P(None, None, "tp"),
            P(None, "tp"),
            P(None, "tp"),
            P(None, "tp"),
            P("tp"),
        ),
        out_specs=(P(None, "tp", "sp", None), P(None, "tp")),
        check_vma=False,
    )
```

```python
import jax
import jax.numpy as jnp
from jax import lax
from jax.experimental import pallas as pl
from jax.experimental.pallas import tpu as pltpu
from jax.sharding import PartitionSpec as P

HD = 64
EPS = 1e-05
EXTRA = 16


def swap_halves(values):
    lanes = values.shape[-1]
    lane = lax.broadcasted_iota(jnp.int32, values.shape, len(values.shape) - 1)
    quarter = HD // 2
    back = pltpu.roll(values, lanes - quarter, len(values.shape) - 1)
    ahead = pltpu.roll(values, quarter, len(values.shape) - 1)
    return jnp.where(lane % HD < quarter, back, ahead)


def state_kernel(
    total_ref,
    new_ref,
    query_ref,
    arrived_ref,
    last_a_ref,
    last_b_ref,
    weight_ref,
    query_weight_ref,
    cos_ref,
    sin_ref,
    decay_ref,
    carried_ref,
    one_ref,
    new_cos_ref,
    new_sin_ref,
    out_ref,
    own_ref,
):
    span_len, inner = decay_ref.shape
    rows = last_a_ref.shape[0]
    prompts = rows // span_len
    groups = out_ref.shape[0]
    keep = HD // groups
    key_scale = HD ** (-0.5)
    lane = lax.broadcasted_iota(jnp.int32, (HD, inner), 1)

    last = jnp.concatenate(
        [last_b_ref[rows + EXTRA : rows + 2 * EXTRA, :], last_b_ref[rows : rows + EXTRA, :]], axis=1
    )
    fresh = new_ref[...] + arrived_ref[rows : rows + EXTRA, :]
    fresh += jnp.dot(last, weight_ref[...], preferred_element_type=jnp.float32)
    query = query_ref[...] + arrived_ref[rows + EXTRA :, :inner]
    query += jnp.dot(last, query_weight_ref[...], preferred_element_type=jnp.float32)
    query = query * new_cos_ref[...] + swap_halves(query) * new_sin_ref[...]
    query = query.astype(jnp.bfloat16).astype(jnp.float32)
    new_key = fresh[:, :inner]
    new_key = (new_key * new_cos_ref[...] + swap_halves(new_key) * new_sin_ref[...]) * key_scale
    new_key = new_key.astype(jnp.bfloat16).astype(jnp.float32)
    new_value = fresh[:, inner:].astype(jnp.bfloat16).astype(jnp.float32)
    products = query * new_key
    new_lane = lax.broadcasted_iota(jnp.int32, products.shape, 1)
    score = jnp.zeros_like(products)
    for h in range(inner // HD):
        here = new_lane // HD == h
        score = jnp.where(
            here, jnp.sum(jnp.where(here, products, 0.0), axis=1, keepdims=True), score
        )
    own_ref[...] = score * new_value
    columns = jnp.transpose(query)

    for s in range(prompts):
        at = pl.ds(s * span_len, span_len)
        last = jnp.concatenate([last_a_ref[at, :], last_b_ref[at, :]], axis=1)
        total = total_ref[at, :] + arrived_ref[at, :]
        total += jnp.dot(last, weight_ref[...], preferred_element_type=jnp.float32)
        keys = total[:, :inner]
        values = total[:, inner:].astype(jnp.bfloat16)
        keys = (keys * cos_ref[...] + swap_halves(keys) * sin_ref[...]).astype(jnp.bfloat16)
        weighted = (keys.astype(jnp.float32) * decay_ref[...]).astype(jnp.bfloat16)
        full = lax.dot_general(
            weighted, values, (((0,), (0,)), ((), ())), preferred_element_type=jnp.float32
        )
        state = jnp.where(lane < HD, full[:HD], full[HD:]) * carried_ref[...]
        entries = jnp.where(lane < HD, columns[:HD, s : s + 1], columns[HD:, s : s + 1])
        read = jnp.sum(state * entries, axis=0, keepdims=True) * one_ref[...]
        for g in range(groups):
            out_ref[g, s * keep : (s + 1) * keep, :] = state[g * keep : (g + 1) * keep]
            out_ref[g, prompts * keep + s : prompts * keep + s + 1, :] = read


def span_states(prompts, groups, decay, *operands):
    inner = decay.shape[1]
    keep = HD // groups
    whole = pl.BlockSpec(memory_space=pltpu.VMEM)
    return pl.pallas_call(
        state_kernel,
        in_specs=[whole] * len(operands),
        out_specs=[whole, whole],
        out_shape=[
            jax.ShapeDtypeStruct((groups, prompts * (keep + 1), inner), jnp.float32),
            jax.ShapeDtypeStruct((EXTRA, inner), jnp.float32),
        ],
        compiler_params=pltpu.CompilerParams(vmem_limit_bytes=24 * 1024 * 1024),
        name="span_states",
    )(*operands)


def finish_kernel(arrived_ref, own_ref, state_ref, read_ref):
    total = jnp.sum(arrived_ref[...], axis=0)
    prompts, heads, keep, _ = state_ref.shape
    for s in range(prompts):
        for h in range(heads):
            state_ref[s, h] = total[s * keep : (s + 1) * keep, h * HD : (h + 1) * HD].astype(
                jnp.bfloat16
            )
    raw = total[prompts * keep :] + own_ref[:prompts, :]
    lane = lax.broadcasted_iota(jnp.int32, raw.shape, 1)

    def per_head(values):
        result = jnp.zeros_like(values)
        for h in range(heads):
            here = lane // HD == h
            mean = jnp.sum(jnp.where(here, values, 0.0), axis=1, keepdims=True) / HD
            result = jnp.where(here, mean, result)
        return result

    centered = raw - per_head(raw)
    spread = per_head(centered * centered)
    read_ref[...] = (centered * lax.rsqrt(spread + EPS)).astype(jnp.bfloat16)


def finish(arrived, own_term, prompts, heads, keep):
    inner = own_term.shape[1]
    whole = pl.BlockSpec(memory_space=pltpu.VMEM)
    return pl.pallas_call(
        finish_kernel,
        in_specs=[whole, whole],
        out_specs=[whole, whole],
        out_shape=[
            jax.ShapeDtypeStruct((prompts, heads, keep, HD), jnp.bfloat16),
            jax.ShapeDtypeStruct((prompts, inner), jnp.bfloat16),
        ],
        compiler_params=pltpu.CompilerParams(vmem_limit_bytes=4 * 1024 * 1024),
        name="finish",
    )(arrived, own_term)


def angles_at(positions, heads):
    half_dim = HD // 2
    inverse = 10000.0 ** (-jnp.arange(half_dim, dtype=jnp.float32) / half_dim)
    angles = positions.astype(jnp.float32)[:, None] * inverse[None, :]
    cosine = jnp.cos(angles)
    sine = jnp.sin(angles)
    cosine = jnp.tile(jnp.concatenate([cosine, cosine], axis=1), (1, heads))
    sine = jnp.tile(jnp.concatenate([-sine, sine], axis=1), (1, heads))
    return cosine, sine


def body(tokens, new_token, query_weight, key_weight, value_weight, log_decay):
    prompts, span_len, width = tokens.shape
    heads = log_decay.shape[0]
    inner = heads * HD
    groups = lax.axis_size("sp")
    own_index = lax.axis_index("sp")
    tp_index = lax.axis_index("tp")
    planes = lax.axis_size("tp") // 2
    plane = tp_index // 2
    core = tp_index % 2
    toward = 1 - 2 * core
    rows = prompts * span_len
    key_scale = HD ** (-0.5)

    partner = [(i, i ^ 1) for i in range(2 * planes)]
    onward = [
        (2 * z + c, 2 * ((z + (1 if c == 0 else -1)) % planes) + c)
        for z in range(planes)
        for c in range(2)
    ]

    def sent(value, pairs):
        return lax.ppermute(value, "tp", pairs)

    chain_a = tokens.reshape(rows, width)
    new_rows = jnp.concatenate(
        [new_token[:, 0], jnp.zeros((EXTRA - prompts, width), new_token.dtype)], axis=0
    )
    other_tokens = sent(chain_a, partner)
    other_rows = sent(new_rows, partner)
    chain_b = jnp.concatenate([other_tokens, other_rows, new_rows], axis=0)

    main_weights = jnp.concatenate([key_weight, value_weight], axis=1)
    all_weights = jnp.concatenate(
        [main_weights, sent(key_weight, partner), sent(value_weight, partner)],
        axis=1,
    ).reshape(2 * planes, width, 4 * inner)
    main_weights = main_weights.reshape(2 * planes, width, 2 * inner)
    own_query = query_weight.reshape(2 * planes, width, inner)
    all_query = jnp.concatenate([query_weight, sent(query_weight, partner)], axis=1)
    all_query = all_query.reshape(2 * planes, width, 2 * inner)

    def places(offset):
        at = (plane - offset * toward) % planes
        return 2 * at + core, 2 * at + 1 - core

    def block(weights, at):
        return lax.dynamic_index_in_dim(weights, at, 0, keepdims=False)

    def project(a, b, offset, weights, queries):
        at_a, at_b = places(offset)

        def both(left, right, table):
            part = jnp.dot(left, block(table, at_a), preferred_element_type=jnp.float32)
            return part + jnp.dot(right, block(table, at_b), preferred_element_type=jnp.float32)

        new_b = b[rows : rows + EXTRA]
        new_a = b[rows + EXTRA :]
        return (
            both(a, b[:rows], weights),
            both(new_a, new_b, weights),
            both(new_a, new_b, queries),
        )

    def added(left, right):
        return tuple(x + y for x, y in zip(left, right))

    own = project(chain_a, chain_b, 0, main_weights, own_query)
    reach = planes // 2
    sums = None
    for step in range(1, reach):
        chain_a = sent(chain_a, onward)
        chain_b = sent(chain_b, onward)
        more = project(chain_a, chain_b, step, all_weights, all_query)
        sums = more if sums is None else added(sums, more)
        sums = lax.optimization_barrier(sums)
    last_a = sent(chain_a, onward)
    last_b = sent(chain_b, onward)

    main, new_main, query = sums
    outgoing = jnp.concatenate(
        [
            main[:, 2 * inner :],
            new_main[:, 2 * inner :],
            jnp.concatenate([query[:, inner:]] * 2, axis=1),
        ],
        axis=0,
    )
    arrived = sent(outgoing, partner)
    own = added(own, (main[:, : 2 * inner], new_main[:, : 2 * inner], query[:, :inner]))
    at_a, at_b = places(reach)
    last_weights = jnp.concatenate([block(main_weights, at_a), block(main_weights, at_b)], axis=0)
    last_query = jnp.concatenate([block(own_query, at_a), block(own_query, at_b)], axis=0)

    local = jnp.arange(span_len, dtype=jnp.int32)
    cosine, sine = angles_at(own_index * span_len + local, heads)
    to_end = (span_len - 1 - local).astype(jnp.float32)
    lane_decay = jnp.repeat(log_decay, HD)
    decay_rows = jnp.exp(to_end[:, None] * lane_decay[None, :])
    distance = (span_len * (groups - 1 - own_index)).astype(jnp.float32)
    carried = jnp.exp(lane_decay * distance)[None, :]
    one = jnp.exp(lane_decay)[None, :]
    new_cosine, new_sine = angles_at(jnp.full((1,), groups * span_len, jnp.int32), heads)

    messages, own_term = span_states(
        prompts,
        groups,
        decay_rows,
        *own,
        arrived,
        last_a,
        last_b,
        last_weights,
        last_query,
        cosine * key_scale,
        sine * key_scale,
        decay_rows,
        carried,
        one,
        new_cosine,
        new_sine,
    )
    arrived = lax.all_to_all(messages, "sp", split_axis=0, concat_axis=0, tiled=True)
    return tuple(finish(arrived, own_term, prompts, heads, HD // groups))


def solution(mesh):
    return jax.shard_map(
        body,
        mesh=mesh,
        in_specs=(
            P(None, "sp", "tp"),
            P(None, None, "tp"),
            P(None, "tp"),
            P(None, "tp"),
            P(None, "tp"),
            P("tp"),
        ),
        out_specs=(P(None, "tp", "sp", None), P(None, "tp")),
        check_vma=False,
    )
```

```python
import functools

import jax
import jax.numpy as jnp
from jax import lax
from jax.experimental import pallas as pl
from jax.experimental.pallas import tpu as pltpu
from jax.sharding import PartitionSpec as P

HD = 64
EPS = 1e-05
EXTRA = 16


def swap_halves(values):
    lanes = values.shape[-1]
    lane = lax.broadcasted_iota(jnp.int32, values.shape, len(values.shape) - 1)
    quarter = HD // 2
    back = pltpu.roll(values, lanes - quarter, len(values.shape) - 1)
    ahead = pltpu.roll(values, quarter, len(values.shape) - 1)
    return jnp.where(lane % HD < quarter, back, ahead)


def row_block(place_ref, offset):
    planes = place_ref[3]
    toward = 1 - 2 * place_ref[1]
    return lax.rem(place_ref[0] - offset * toward + planes, planes)


def at_rows(block, width):
    return pl.ds(pl.multiple_of(block * width, width), width)


def stacked(place_ref, weight_ref, offsets, width):
    core = place_ref[1]
    blocks = []
    for offset in offsets:
        plane = row_block(place_ref, offset)
        blocks.append(weight_ref[at_rows(2 * plane + core, width), :])
        blocks.append(weight_ref[at_rows(2 * plane + 1 - core, width), :])
    return jnp.concatenate(blocks, axis=0)


def sums_kernel(offsets, span_len, place_ref, own_w_ref, other_w_ref, *refs):
    count = len(offsets)
    a_refs, b_refs, rest = refs[:count], refs[count : 2 * count], refs[2 * count :]
    own_ref, other_ref = rest[-2:]
    before = rest[:-2]
    rows, width = a_refs[0].shape
    inner = own_ref.shape[1]
    hops = [i for i in range(count) if offsets[i] > 0]
    own_plane = [i for i in range(count) if offsets[i] == 0]

    def step(s, carry):
        at = pl.ds(pl.multiple_of(s * span_len, span_len), span_len)

        def gathered(which):
            pieces = []
            for i in which:
                pieces += [a_refs[i][at, :], b_refs[i][at, :]]
            return jnp.concatenate(pieces, axis=1)

        weights = jnp.concatenate(
            [
                stacked(place_ref, own_w_ref, [offsets[i] for i in hops], width),
                stacked(place_ref, other_w_ref, [offsets[i] for i in hops], width),
            ],
            axis=1,
        )
        part = jnp.dot(gathered(hops), weights, preferred_element_type=jnp.float32)
        own, other = part[:, :inner], part[:, inner:]
        if own_plane:
            here = stacked(place_ref, own_w_ref, [0], width)
            own += jnp.dot(gathered(own_plane), here, preferred_element_type=jnp.float32)
        if before:
            own += before[0][at, :]
            other += before[1][at, :]
        own_ref[at, :] = own
        other_ref[at, :] = other
        return carry

    lax.fori_loop(0, rows // span_len, step, 0)


def ring_sums(offsets, span_len, place, own_weights, other_weights, a_list, b_list, before):
    rows, width = a_list[0].shape
    inner = own_weights.shape[1]
    whole = pl.BlockSpec(memory_space=pltpu.VMEM)
    operands = [own_weights, other_weights, *a_list, *b_list, *before]
    flops = 2 * rows * 2 * inner * 2 * width * len(offsets)
    return pl.pallas_call(
        functools.partial(sums_kernel, offsets, span_len),
        in_specs=[pl.BlockSpec(memory_space=pltpu.SMEM)] + [whole] * len(operands),
        out_specs=[whole, whole],
        out_shape=[jax.ShapeDtypeStruct((rows, inner), jnp.float32)] * 2,
        compiler_params=pltpu.CompilerParams(vmem_limit_bytes=16 * 1024 * 1024),
        cost_estimate=pl.CostEstimate(flops=flops, bytes_accessed=0, transcendentals=0),
        name="ring_sums",
    )(place, *operands)


def state_kernel(
    place_ref,
    total_ref,
    arrived_ref,
    here_new_ref,
    mine_new_ref,
    theirs_new_ref,
    last_a_ref,
    last_b_ref,
    main_ref,
    query_w_ref,
    cos_ref,
    sin_ref,
    lane_ref,
    out_ref,
    own_ref,
):
    rows, width = last_a_ref.shape
    inner = query_w_ref.shape[1]
    groups, out_rows, _ = out_ref.shape
    keep = HD // groups
    prompts = out_rows // (keep + 1)
    span_len = rows // prompts
    reach = mine_new_ref.shape[0] // (2 * EXTRA) + 1
    lane = lax.broadcasted_iota(jnp.int32, (HD, inner), 1)
    lane_decay = lane_ref[...]
    distance = ((groups - 1 - place_ref[2]) * span_len).astype(jnp.float32)
    carried = jnp.exp(lane_decay * distance)
    one = jnp.exp(lane_decay)
    to_end = lax.broadcasted_iota(jnp.int32, (span_len, inner), 0)
    decay = jnp.exp((span_len - 1 - to_end).astype(jnp.float32) * lane_decay)

    def pair(ref, start):
        return [ref[start : start + EXTRA, :], ref[start + EXTRA : start + 2 * EXTRA, :]]

    pieces = pair(here_new_ref, 0)
    order = [0]
    for k in range(1, reach):
        pieces += pair(mine_new_ref, (k - 1) * 2 * EXTRA)
        pieces += pair(theirs_new_ref, (k - 1) * 2 * EXTRA)
        order += [k, -k]
    pieces += pair(last_b_ref, rows)
    order.append(reach)
    entries = jnp.concatenate(pieces, axis=1)
    plane_rows = [at_rows(row_block(place_ref, k), 2 * width) for k in order]
    weights = jnp.concatenate(
        [jnp.concatenate([main_ref[at, :], query_w_ref[at, :]], axis=1) for at in plane_rows], axis=0
    )
    fresh = jnp.dot(entries, weights, preferred_element_type=jnp.float32)
    new_cos = cos_ref[span_len : span_len + 1, :]
    new_sin = sin_ref[span_len : span_len + 1, :]
    new_key = fresh[:, :inner]
    new_key = new_key * new_cos + swap_halves(new_key) * new_sin
    new_key = new_key.astype(jnp.bfloat16).astype(jnp.float32)
    new_value = fresh[:, inner : 2 * inner].astype(jnp.bfloat16).astype(jnp.float32)
    query = fresh[:, 2 * inner :]
    query = (query * new_cos + swap_halves(query) * new_sin) * (HD**0.5)
    query = query.astype(jnp.bfloat16).astype(jnp.float32)
    products = query * new_key
    new_lane = lax.broadcasted_iota(jnp.int32, products.shape, 1)
    score = jnp.zeros_like(products)
    for h in range(inner // HD):
        here = new_lane // HD == h
        score = jnp.where(
            here, jnp.sum(jnp.where(here, products, 0.0), axis=1, keepdims=True), score
        )
    own_ref[...] = score * new_value
    columns = jnp.transpose(query)

    last_weights = stacked(place_ref, main_ref, [reach], width)
    cosine = cos_ref[:span_len, :]
    sine = sin_ref[:span_len, :]
    for s in range(prompts):
        at = pl.ds(s * span_len, span_len)
        last = jnp.concatenate([last_a_ref[at, :], last_b_ref[at, :]], axis=1)
        total = total_ref[at, :] + arrived_ref[at, :]
        total += jnp.dot(last, last_weights, preferred_element_type=jnp.float32)
        keys = total[:, :inner]
        values = total[:, inner:].astype(jnp.bfloat16)
        keys = (keys * cosine + swap_halves(keys) * sine).astype(jnp.bfloat16)
        weighted = (keys.astype(jnp.float32) * decay).astype(jnp.bfloat16)
        full = lax.dot_general(
            weighted, values, (((0,), (0,)), ((), ())), preferred_element_type=jnp.float32
        )
        state = jnp.where(lane < HD, full[:HD], full[HD:]) * carried
        column = jnp.where(lane < HD, columns[:HD, s : s + 1], columns[HD:, s : s + 1])
        read = jnp.sum(state * column, axis=0, keepdims=True) * one
        for g in range(groups):
            out_ref[g, s * keep : (s + 1) * keep, :] = state[g * keep : (g + 1) * keep]
            out_ref[g, prompts * keep + s : prompts * keep + s + 1, :] = read


def span_states(prompts, groups, inner, place, *operands):
    keep = HD // groups
    whole = pl.BlockSpec(memory_space=pltpu.VMEM)
    return pl.pallas_call(
        state_kernel,
        in_specs=[pl.BlockSpec(memory_space=pltpu.SMEM)] + [whole] * len(operands),
        out_specs=[whole, whole],
        out_shape=[
            jax.ShapeDtypeStruct((groups, prompts * (keep + 1), inner), jnp.float32),
            jax.ShapeDtypeStruct((EXTRA, inner), jnp.float32),
        ],
        compiler_params=pltpu.CompilerParams(vmem_limit_bytes=24 * 1024 * 1024),
        name="span_states",
    )(place, *operands)


def finish_kernel(arrived_ref, own_ref, state_ref, read_ref):
    total = jnp.sum(arrived_ref[...], axis=0)
    prompts, heads, keep, _ = state_ref.shape
    for s in range(prompts):
        for h in range(heads):
            state_ref[s, h] = total[s * keep : (s + 1) * keep, h * HD : (h + 1) * HD].astype(
                jnp.bfloat16
            )
    raw = total[prompts * keep :] + own_ref[:prompts, :]
    lane = lax.broadcasted_iota(jnp.int32, raw.shape, 1)

    def per_head(values):
        result = jnp.zeros_like(values)
        for h in range(heads):
            here = lane // HD == h
            mean = jnp.sum(jnp.where(here, values, 0.0), axis=1, keepdims=True) / HD
            result = jnp.where(here, mean, result)
        return result

    centered = raw - per_head(raw)
    spread = per_head(centered * centered)
    read_ref[...] = (centered * lax.rsqrt(spread + EPS)).astype(jnp.bfloat16)


def finish(arrived, own_term, prompts, heads, keep):
    inner = own_term.shape[1]
    whole = pl.BlockSpec(memory_space=pltpu.VMEM)
    return pl.pallas_call(
        finish_kernel,
        in_specs=[whole, whole],
        out_specs=[whole, whole],
        out_shape=[
            jax.ShapeDtypeStruct((prompts, heads, keep, HD), jnp.bfloat16),
            jax.ShapeDtypeStruct((prompts, inner), jnp.bfloat16),
        ],
        compiler_params=pltpu.CompilerParams(vmem_limit_bytes=4 * 1024 * 1024),
        name="finish",
    )(arrived, own_term)


def tables(first_position, span_len, new_position, heads):
    quarter = HD // 2
    lane = jnp.arange(heads * HD, dtype=jnp.int32)
    inverse = 10000.0 ** (-(lane % quarter).astype(jnp.float32) / quarter)
    row = jnp.arange(span_len + 8, dtype=jnp.int32)
    position = jnp.where(row < span_len, first_position + row, new_position).astype(jnp.float32)
    angles = position[:, None] * inverse[None, :]
    key_scale = HD ** (-0.5)
    sign = jnp.where(lane % HD < quarter, -key_scale, key_scale)
    return jnp.cos(angles) * key_scale, jnp.sin(angles) * sign[None, :]


def body(tokens, new_token, query_weight, key_weight, value_weight, log_decay):
    prompts, span_len, width = tokens.shape
    heads = log_decay.shape[0]
    inner = heads * HD
    groups = lax.axis_size("sp")
    own_index = lax.axis_index("sp")
    tp_index = lax.axis_index("tp")
    planes = lax.axis_size("tp") // 2
    reach = planes // 2
    plane = tp_index // 2
    core = tp_index % 2
    rows = prompts * span_len
    place = jnp.stack([plane, core, own_index, jnp.int32(planes)]).astype(jnp.int32)

    partner = [(i, i ^ 1) for i in range(2 * planes)]
    onward = [
        (2 * z + c, 2 * ((z + (1 if c == 0 else -1)) % planes) + c)
        for z in range(planes)
        for c in range(2)
    ]

    def sent(value, pairs):
        return lax.ppermute(value, "tp", pairs)

    chain_a = tokens.reshape(rows, width)
    new_rows = jnp.concatenate(
        [new_token[:, 0], jnp.zeros((EXTRA - prompts, width), new_token.dtype)], axis=0
    )
    other_tokens = sent(chain_a, partner)
    other_rows = sent(new_rows, partner)
    new_pair = jnp.concatenate(
        [
            jnp.where(core == 0, new_rows, other_rows),
            jnp.where(core == 0, other_rows, new_rows),
        ],
        axis=0,
    )
    chain_b = jnp.concatenate([other_tokens, new_pair], axis=0)
    main_weights = jnp.concatenate([key_weight, value_weight], axis=1)
    other_weights = sent(main_weights, partner)
    cosine, sine = tables(own_index * span_len, span_len, groups * span_len, heads)
    lane_decay = jnp.repeat(log_decay, HD)[None, :]

    a_list, b_list = [chain_a], [other_tokens]
    new_list = []
    for step in range(1, reach + 1):
        chain_a = sent(chain_a, onward)
        chain_b = sent(chain_b, onward)
        if step == 1:
            chain_a, cosine, sine, lane_decay = lax.optimization_barrier(
                (chain_a, cosine, sine, lane_decay)
            )
        a_list.append(chain_a)
        b_list.append(chain_b)
        new_list.append(chain_b[rows:])
    sums = ()
    for low, high in ((0, 4), (4, 7), (7, 8)):
        sums = ring_sums(
            tuple(range(low, high)),
            span_len,
            place,
            main_weights,
            other_weights,
            a_list[low:high],
            b_list[low:high],
            sums,
        )
    own, other = sums

    arrived = sent(other, partner)
    mine_new = jnp.concatenate(new_list[:-1], axis=0)
    theirs_new = sent(mine_new, partner)

    messages, own_term = span_states(
        prompts,
        groups,
        inner,
        place,
        own,
        arrived,
        new_pair,
        mine_new,
        theirs_new,
        a_list[-1],
        b_list[-1],
        main_weights,
        query_weight,
        cosine,
        sine,
        lane_decay,
    )
    arrived = lax.all_to_all(messages, "sp", split_axis=0, concat_axis=0, tiled=True)
    return tuple(finish(arrived, own_term, prompts, heads, HD // groups))


def solution(mesh):
    return jax.shard_map(
        body,
        mesh=mesh,
        in_specs=(
            P(None, "sp", "tp"),
            P(None, None, "tp"),
            P(None, "tp"),
            P(None, "tp"),
            P(None, "tp"),
            P("tp"),
        ),
        out_specs=(P(None, "tp", "sp", None), P(None, "tp")),
        check_vma=False,
    )
```

```python
import functools

import jax
import jax.numpy as jnp
from jax import lax
from jax.experimental import pallas as pl
from jax.experimental.pallas import tpu as pltpu
from jax.sharding import PartitionSpec as P

HD = 64
EPS = 1e-05
EXTRA = 16


def swap_halves(values):
    lanes = values.shape[-1]
    lane = lax.broadcasted_iota(jnp.int32, values.shape, len(values.shape) - 1)
    quarter = HD // 2
    back = pltpu.roll(values, lanes - quarter, len(values.shape) - 1)
    ahead = pltpu.roll(values, quarter, len(values.shape) - 1)
    return jnp.where(lane % HD < quarter, back, ahead)


def row_block(place_ref, offset):
    planes = place_ref[3]
    toward = 1 - 2 * place_ref[1]
    return lax.rem(place_ref[0] - offset * toward + planes, planes)


def at_rows(block, width):
    return pl.ds(pl.multiple_of(block * width, width), width)


def stacked(place_ref, weight_ref, offsets, width):
    core = place_ref[1]
    blocks = []
    for offset in offsets:
        plane = row_block(place_ref, offset)
        blocks.append(weight_ref[at_rows(2 * plane + core, width), :])
        blocks.append(weight_ref[at_rows(2 * plane + 1 - core, width), :])
    return jnp.concatenate(blocks, axis=0)


def sums_kernel(offsets, span_len, has_before, place_ref, own_w_ref, other_w_ref, *refs):
    count = len(offsets)
    a_refs, b_refs, rest = refs[:count], refs[count : 2 * count], refs[2 * count :]
    before = rest[:2] if has_before else ()
    own_ref, other_ref, held, landed = rest[len(before) :]
    rows, width = a_refs[0].shape
    core = place_ref[1]
    hops = [i for i in range(count) if offsets[i] > 0]

    copies = []
    for j, i in enumerate(hops):
        plane = row_block(place_ref, offsets[i])
        for side, block in enumerate((2 * plane + core, 2 * plane + 1 - core)):
            slot = 2 * j + side
            copies.append(
                pltpu.make_async_copy(
                    other_w_ref.at[at_rows(block, width), :],
                    held.at[pl.ds(slot * width, width), :],
                    landed.at[slot],
                )
            )
    for copy in copies:
        copy.start()

    def summed(out_ref, earlier, which, weights_of):
        def step(s, carry):
            at = pl.ds(pl.multiple_of(s * span_len, span_len), span_len)
            pieces = []
            for i in which:
                pieces += [a_refs[i][at, :], b_refs[i][at, :]]
            both = jnp.concatenate(pieces, axis=1)
            part = jnp.dot(both, weights_of(), preferred_element_type=jnp.float32)
            if earlier is not None:
                part += earlier[at, :]
            out_ref[at, :] = part
            return carry

        lax.fori_loop(0, rows // span_len, step, 0)

    summed(
        own_ref,
        before[0] if before else None,
        list(range(count)),
        lambda: stacked(place_ref, own_w_ref, offsets, width),
    )
    for copy in copies:
        copy.wait()
    summed(other_ref, before[1] if before else None, hops, lambda: held[...])


def ring_sums(offsets, span_len, place, own_weights, other_weights, a_list, b_list, before):
    rows, width = a_list[0].shape
    inner = own_weights.shape[1]
    whole = pl.BlockSpec(memory_space=pltpu.VMEM)
    operands = [*a_list, *b_list, *before]
    blocks = 2 * sum(1 for offset in offsets if offset > 0)
    flops = 2 * rows * 2 * inner * 2 * width * len(offsets)
    return pl.pallas_call(
        functools.partial(sums_kernel, offsets, span_len, bool(before)),
        in_specs=[
            pl.BlockSpec(memory_space=pltpu.SMEM),
            whole,
            pl.BlockSpec(memory_space=pltpu.HBM),
        ]
        + [whole] * len(operands),
        out_specs=[whole, whole],
        out_shape=[jax.ShapeDtypeStruct((rows, inner), jnp.float32)] * 2,
        scratch_shapes=[
            pltpu.VMEM((blocks * width, inner), own_weights.dtype),
            pltpu.SemaphoreType.DMA((blocks,)),
        ],
        compiler_params=pltpu.CompilerParams(vmem_limit_bytes=16 * 1024 * 1024),
        cost_estimate=pl.CostEstimate(flops=flops, bytes_accessed=0, transcendentals=0),
        name="ring_sums",
    )(place, own_weights, other_weights, *operands)


def state_kernel(
    place_ref,
    total_ref,
    arrived_ref,
    here_new_ref,
    mine_new_ref,
    theirs_new_ref,
    last_a_ref,
    last_b_ref,
    main_ref,
    query_w_ref,
    cos_ref,
    sin_ref,
    lane_ref,
    out_ref,
    own_ref,
):
    rows, width = last_a_ref.shape
    inner = query_w_ref.shape[1]
    groups, out_rows, _ = out_ref.shape
    keep = HD // groups
    prompts = out_rows // (keep + 1)
    span_len = rows // prompts
    reach = mine_new_ref.shape[0] // (2 * EXTRA) + 1
    lane = lax.broadcasted_iota(jnp.int32, (HD, inner), 1)
    lane_decay = lane_ref[...]
    distance = ((groups - 1 - place_ref[2]) * span_len).astype(jnp.float32)
    carried = jnp.exp(lane_decay * distance)
    one = jnp.exp(lane_decay)
    to_end = lax.broadcasted_iota(jnp.int32, (span_len, inner), 0)
    decay = jnp.exp((span_len - 1 - to_end).astype(jnp.float32) * lane_decay)

    def pair(ref, start):
        return [ref[start : start + EXTRA, :], ref[start + EXTRA : start + 2 * EXTRA, :]]

    pieces = pair(here_new_ref, 0)
    order = [0]
    for k in range(1, reach):
        pieces += pair(mine_new_ref, (k - 1) * 2 * EXTRA)
        pieces += pair(theirs_new_ref, (k - 1) * 2 * EXTRA)
        order += [k, -k]
    pieces += pair(last_b_ref, rows)
    order.append(reach)
    entries = jnp.concatenate(pieces, axis=1)
    plane_rows = [at_rows(row_block(place_ref, k), 2 * width) for k in order]
    weights = jnp.concatenate(
        [jnp.concatenate([main_ref[at, :], query_w_ref[at, :]], axis=1) for at in plane_rows], axis=0
    )
    fresh = jnp.dot(entries, weights, preferred_element_type=jnp.float32)
    new_cos = cos_ref[span_len : span_len + 1, :]
    new_sin = sin_ref[span_len : span_len + 1, :]
    new_key = fresh[:, :inner]
    new_key = new_key * new_cos + swap_halves(new_key) * new_sin
    new_key = new_key.astype(jnp.bfloat16).astype(jnp.float32)
    new_value = fresh[:, inner : 2 * inner].astype(jnp.bfloat16).astype(jnp.float32)
    query = fresh[:, 2 * inner :]
    query = (query * new_cos + swap_halves(query) * new_sin) * (HD**0.5)
    query = query.astype(jnp.bfloat16).astype(jnp.float32)
    products = query * new_key
    new_lane = lax.broadcasted_iota(jnp.int32, products.shape, 1)
    score = jnp.zeros_like(products)
    for h in range(inner // HD):
        here = new_lane // HD == h
        score = jnp.where(
            here, jnp.sum(jnp.where(here, products, 0.0), axis=1, keepdims=True), score
        )
    own_ref[...] = score * new_value
    columns = jnp.transpose(query)

    last_weights = stacked(place_ref, main_ref, [reach], width)
    cosine = cos_ref[:span_len, :]
    sine = sin_ref[:span_len, :]
    for s in range(prompts):
        at = pl.ds(s * span_len, span_len)
        last = jnp.concatenate([last_a_ref[at, :], last_b_ref[at, :]], axis=1)
        total = total_ref[at, :] + arrived_ref[at, :]
        total += jnp.dot(last, last_weights, preferred_element_type=jnp.float32)
        keys = total[:, :inner]
        values = total[:, inner:].astype(jnp.bfloat16)
        keys = (keys * cosine + swap_halves(keys) * sine).astype(jnp.bfloat16)
        weighted = (keys.astype(jnp.float32) * decay).astype(jnp.bfloat16)
        full = lax.dot_general(
            weighted, values, (((0,), (0,)), ((), ())), preferred_element_type=jnp.float32
        )
        state = jnp.where(lane < HD, full[:HD], full[HD:]) * carried
        column = jnp.where(lane < HD, columns[:HD, s : s + 1], columns[HD:, s : s + 1])
        read = jnp.sum(state * column, axis=0, keepdims=True) * one
        for g in range(groups):
            out_ref[g, s * keep : (s + 1) * keep, :] = state[g * keep : (g + 1) * keep]
            out_ref[g, prompts * keep + s : prompts * keep + s + 1, :] = read


def span_states(prompts, groups, inner, place, *operands):
    keep = HD // groups
    whole = pl.BlockSpec(memory_space=pltpu.VMEM)
    return pl.pallas_call(
        state_kernel,
        in_specs=[pl.BlockSpec(memory_space=pltpu.SMEM)] + [whole] * len(operands),
        out_specs=[whole, whole],
        out_shape=[
            jax.ShapeDtypeStruct((groups, prompts * (keep + 1), inner), jnp.float32),
            jax.ShapeDtypeStruct((EXTRA, inner), jnp.float32),
        ],
        compiler_params=pltpu.CompilerParams(vmem_limit_bytes=24 * 1024 * 1024),
        name="span_states",
    )(place, *operands)


def finish_kernel(arrived_ref, own_ref, state_ref, read_ref):
    total = jnp.sum(arrived_ref[...], axis=0)
    prompts, heads, keep, _ = state_ref.shape
    for s in range(prompts):
        for h in range(heads):
            state_ref[s, h] = total[s * keep : (s + 1) * keep, h * HD : (h + 1) * HD].astype(
                jnp.bfloat16
            )
    raw = total[prompts * keep :] + own_ref[:prompts, :]
    lane = lax.broadcasted_iota(jnp.int32, raw.shape, 1)

    def per_head(values):
        result = jnp.zeros_like(values)
        for h in range(heads):
            here = lane // HD == h
            mean = jnp.sum(jnp.where(here, values, 0.0), axis=1, keepdims=True) / HD
            result = jnp.where(here, mean, result)
        return result

    centered = raw - per_head(raw)
    spread = per_head(centered * centered)
    read_ref[...] = (centered * lax.rsqrt(spread + EPS)).astype(jnp.bfloat16)


def finish(arrived, own_term, prompts, heads, keep):
    inner = own_term.shape[1]
    whole = pl.BlockSpec(memory_space=pltpu.VMEM)
    return pl.pallas_call(
        finish_kernel,
        in_specs=[whole, whole],
        out_specs=[whole, whole],
        out_shape=[
            jax.ShapeDtypeStruct((prompts, heads, keep, HD), jnp.bfloat16),
            jax.ShapeDtypeStruct((prompts, inner), jnp.bfloat16),
        ],
        compiler_params=pltpu.CompilerParams(vmem_limit_bytes=4 * 1024 * 1024),
        name="finish",
    )(arrived, own_term)


def tables(first_position, span_len, new_position, heads):
    quarter = HD // 2
    lane = jnp.arange(heads * HD, dtype=jnp.int32)
    inverse = 10000.0 ** (-(lane % quarter).astype(jnp.float32) / quarter)
    row = jnp.arange(span_len + 8, dtype=jnp.int32)
    position = jnp.where(row < span_len, first_position + row, new_position).astype(jnp.float32)
    angles = position[:, None] * inverse[None, :]
    key_scale = HD ** (-0.5)
    sign = jnp.where(lane % HD < quarter, -key_scale, key_scale)
    return jnp.cos(angles) * key_scale, jnp.sin(angles) * sign[None, :]


def body(tokens, new_token, query_weight, key_weight, value_weight, log_decay):
    prompts, span_len, width = tokens.shape
    heads = log_decay.shape[0]
    inner = heads * HD
    groups = lax.axis_size("sp")
    own_index = lax.axis_index("sp")
    tp_index = lax.axis_index("tp")
    planes = lax.axis_size("tp") // 2
    reach = planes // 2
    plane = tp_index // 2
    core = tp_index % 2
    rows = prompts * span_len
    place = jnp.stack([plane, core, own_index, jnp.int32(planes)]).astype(jnp.int32)

    partner = [(i, i ^ 1) for i in range(2 * planes)]
    onward = [
        (2 * z + c, 2 * ((z + (1 if c == 0 else -1)) % planes) + c)
        for z in range(planes)
        for c in range(2)
    ]

    across = [
        (2 * z + 1 - c, 2 * ((z + (1 if c == 0 else -1)) % planes) + c)
        for z in range(planes)
        for c in range(2)
    ]

    def sent(value, pairs):
        return lax.ppermute(value, "tp", pairs)

    tokens = tokens.reshape(rows, width)
    chain_a = sent(tokens, onward)
    chain_b = sent(tokens, across)
    fresh = new_token[:, 0]
    other_fresh = sent(new_token, partner)[:, 0]
    padding = jnp.zeros((EXTRA - prompts, width), new_token.dtype)
    new_pair = jnp.concatenate(
        [
            jnp.where(core == 0, fresh, other_fresh),
            padding,
            jnp.where(core == 0, other_fresh, fresh),
            padding,
        ],
        axis=0,
    )
    new_first = sent(new_pair, onward)
    main_weights = jnp.concatenate([key_weight, value_weight], axis=1)
    other_weights = sent(main_weights, partner)
    other_tokens = sent(tokens, partner)
    cosine, sine = tables(own_index * span_len, span_len, groups * span_len, heads)
    lane_decay = jnp.repeat(log_decay, HD)[None, :]
    chain_a, cosine, sine, lane_decay = lax.optimization_barrier(
        (chain_a, cosine, sine, lane_decay)
    )

    a_list, b_list = [tokens, chain_a], [other_tokens, chain_b]
    new_list = [new_first]
    chain_b = jnp.concatenate([chain_b, new_first], axis=0)
    for _ in range(2, reach + 1):
        chain_a = sent(chain_a, onward)
        chain_b = sent(chain_b, onward)
        a_list.append(chain_a)
        b_list.append(chain_b)
        new_list.append(chain_b[rows:])
    sums = ()
    for offsets in ((1, 2), (0, 3, 4), (5, 6), (7,)):
        sums = ring_sums(
            offsets,
            span_len,
            place,
            main_weights,
            other_weights,
            [a_list[k] for k in offsets],
            [b_list[k] for k in offsets],
            sums,
        )
    own, other = sums

    arrived = sent(other, partner)
    mine_new = jnp.concatenate(new_list[:-1], axis=0)
    theirs_new = sent(mine_new, partner)

    messages, own_term = span_states(
        prompts,
        groups,
        inner,
        place,
        own,
        arrived,
        new_pair,
        mine_new,
        theirs_new,
        a_list[-1],
        b_list[-1],
        main_weights,
        query_weight,
        cosine,
        sine,
        lane_decay,
    )
    arrived = lax.all_to_all(messages, "sp", split_axis=0, concat_axis=0, tiled=True)
    return tuple(finish(arrived, own_term, prompts, heads, HD // groups))


def solution(mesh):
    return jax.shard_map(
        body,
        mesh=mesh,
        in_specs=(
            P(None, "sp", "tp"),
            P(None, None, "tp"),
            P(None, "tp"),
            P(None, "tp"),
            P(None, "tp"),
            P("tp"),
        ),
        out_specs=(P(None, "tp", "sp", None), P(None, "tp")),
        check_vma=False,
    )
```

```python
import functools

import jax
import jax.numpy as jnp
from jax import lax
from jax.experimental import pallas as pl
from jax.experimental.pallas import tpu as pltpu
from jax.sharding import PartitionSpec as P

HD = 64
EPS = 1e-05
EXTRA = 16


def swap_halves(values):
    lanes = values.shape[-1]
    lane = lax.broadcasted_iota(jnp.int32, values.shape, len(values.shape) - 1)
    quarter = HD // 2
    back = pltpu.roll(values, lanes - quarter, len(values.shape) - 1)
    ahead = pltpu.roll(values, quarter, len(values.shape) - 1)
    return jnp.where(lane % HD < quarter, back, ahead)


def beside_kernel(left_ref, right_ref, out_ref):
    width = left_ref.shape[1]
    out_ref[:, :width] = left_ref[...]
    out_ref[:, width:] = right_ref[...]


def beside(left, right):
    rows, width = left.shape
    whole = pl.BlockSpec(memory_space=pltpu.VMEM)
    return pl.pallas_call(
        beside_kernel,
        in_specs=[whole, whole],
        out_specs=whole,
        out_shape=jax.ShapeDtypeStruct((rows, 2 * width), left.dtype),
        compiler_params=pltpu.CompilerParams(vmem_limit_bytes=6 * 1024 * 1024),
        cost_estimate=pl.CostEstimate(flops=10**8, bytes_accessed=0, transcendentals=0),
        name="beside",
    )(left, right)


def row_block(place_ref, offset):
    planes = place_ref[3]
    toward = 1 - 2 * place_ref[1]
    return lax.rem(place_ref[0] - offset * toward + planes, planes)


def at_rows(block, width):
    return pl.ds(pl.multiple_of(block * width, width), width)


def stacked(place_ref, weight_ref, offsets, width):
    core = place_ref[1]
    blocks = []
    for offset in offsets:
        plane = row_block(place_ref, offset)
        blocks.append(weight_ref[at_rows(2 * plane + core, width), :])
        blocks.append(weight_ref[at_rows(2 * plane + 1 - core, width), :])
    return jnp.concatenate(blocks, axis=0)


def sums_kernel(offsets, span_len, has_before, place_ref, own_w_ref, other_w_ref, *refs):
    count = len(offsets)
    a_refs, b_refs, rest = refs[:count], refs[count : 2 * count], refs[2 * count :]
    before = rest[:2] if has_before else ()
    own_ref, other_ref, held, landed = rest[len(before) :]
    rows, width = a_refs[0].shape
    core = place_ref[1]
    hops = [i for i in range(count) if offsets[i] > 0]

    copies = []
    for j, i in enumerate(hops):
        plane = row_block(place_ref, offsets[i])
        for side, block in enumerate((2 * plane + core, 2 * plane + 1 - core)):
            slot = 2 * j + side
            copies.append(
                pltpu.make_async_copy(
                    other_w_ref.at[at_rows(block, width), :],
                    held.at[pl.ds(slot * width, width), :],
                    landed.at[slot],
                )
            )
    for copy in copies:
        copy.start()

    def summed(out_ref, earlier, which, weights_of):
        def step(s, carry):
            at = pl.ds(pl.multiple_of(s * span_len, span_len), span_len)
            pieces = []
            for i in which:
                pieces += [a_refs[i][at, :], b_refs[i][at, :]]
            both = jnp.concatenate(pieces, axis=1)
            part = jnp.dot(both, weights_of(), preferred_element_type=jnp.float32)
            if earlier is not None:
                part += earlier[at, :]
            out_ref[at, :] = part
            return carry

        lax.fori_loop(0, rows // span_len, step, 0)

    summed(
        own_ref,
        before[0] if before else None,
        list(range(count)),
        lambda: stacked(place_ref, own_w_ref, offsets, width),
    )
    for copy in copies:
        copy.wait()
    summed(other_ref, before[1] if before else None, hops, lambda: held[...])


def ring_sums(offsets, span_len, place, own_weights, other_weights, a_list, b_list, before):
    rows, width = a_list[0].shape
    inner = own_weights.shape[1]
    whole = pl.BlockSpec(memory_space=pltpu.VMEM)
    operands = [*a_list, *b_list, *before]
    blocks = 2 * sum(1 for offset in offsets if offset > 0)
    flops = 2 * rows * 2 * inner * 2 * width * len(offsets)
    return pl.pallas_call(
        functools.partial(sums_kernel, offsets, span_len, bool(before)),
        in_specs=[
            pl.BlockSpec(memory_space=pltpu.SMEM),
            whole,
            pl.BlockSpec(memory_space=pltpu.HBM),
        ]
        + [whole] * len(operands),
        out_specs=[whole, whole],
        out_shape=[jax.ShapeDtypeStruct((rows, inner), jnp.float32)] * 2,
        scratch_shapes=[
            pltpu.VMEM((blocks * width, inner), own_weights.dtype),
            pltpu.SemaphoreType.DMA((blocks,)),
        ],
        compiler_params=pltpu.CompilerParams(vmem_limit_bytes=6 * 1024 * 1024),
        cost_estimate=pl.CostEstimate(flops=flops, bytes_accessed=0, transcendentals=0),
        name="ring_sums",
    )(place, own_weights, other_weights, *operands)


def state_kernel(
    place_ref,
    total_ref,
    arrived_ref,
    here_new_ref,
    mine_new_ref,
    theirs_new_ref,
    last_a_ref,
    last_b_ref,
    main_ref,
    query_w_ref,
    cos_ref,
    sin_ref,
    lane_ref,
    out_ref,
    own_ref,
):
    rows, width = last_a_ref.shape
    inner = query_w_ref.shape[1]
    groups, out_rows, _ = out_ref.shape
    keep = HD // groups
    prompts = out_rows // (keep + 1)
    span_len = rows // prompts
    reach = mine_new_ref.shape[0] // (2 * EXTRA) + 1
    lane = lax.broadcasted_iota(jnp.int32, (HD, inner), 1)
    lane_decay = lane_ref[...]
    distance = ((groups - 1 - place_ref[2]) * span_len).astype(jnp.float32)
    carried = jnp.exp(lane_decay * distance)
    one = jnp.exp(lane_decay)
    to_end = lax.broadcasted_iota(jnp.int32, (span_len, inner), 0)
    decay = jnp.exp((span_len - 1 - to_end).astype(jnp.float32) * lane_decay)

    def pair(ref, start):
        return [ref[start : start + EXTRA, :], ref[start + EXTRA : start + 2 * EXTRA, :]]

    pieces = pair(here_new_ref, 0)
    order = [0]
    for k in range(1, reach):
        pieces += pair(mine_new_ref, (k - 1) * 2 * EXTRA)
        pieces += pair(theirs_new_ref, (k - 1) * 2 * EXTRA)
        order += [k, -k]
    pieces += pair(last_b_ref, rows)
    order.append(reach)
    entries = jnp.concatenate(pieces, axis=1)
    plane_rows = [at_rows(row_block(place_ref, k), 2 * width) for k in order]
    weights = jnp.concatenate(
        [jnp.concatenate([main_ref[at, :], query_w_ref[at, :]], axis=1) for at in plane_rows], axis=0
    )
    fresh = jnp.dot(entries, weights, preferred_element_type=jnp.float32)
    new_cos = cos_ref[span_len : span_len + 1, :]
    new_sin = sin_ref[span_len : span_len + 1, :]
    new_key = fresh[:, :inner]
    new_key = new_key * new_cos + swap_halves(new_key) * new_sin
    new_key = new_key.astype(jnp.bfloat16).astype(jnp.float32)
    new_value = fresh[:, inner : 2 * inner].astype(jnp.bfloat16).astype(jnp.float32)
    query = fresh[:, 2 * inner :]
    query = (query * new_cos + swap_halves(query) * new_sin) * (HD**0.5)
    query = query.astype(jnp.bfloat16).astype(jnp.float32)
    products = query * new_key
    new_lane = lax.broadcasted_iota(jnp.int32, products.shape, 1)
    score = jnp.zeros_like(products)
    for h in range(inner // HD):
        here = new_lane // HD == h
        score = jnp.where(
            here, jnp.sum(jnp.where(here, products, 0.0), axis=1, keepdims=True), score
        )
    own_ref[...] = score * new_value
    columns = jnp.transpose(query)

    last_weights = stacked(place_ref, main_ref, [reach], width)
    cosine = cos_ref[:span_len, :]
    sine = sin_ref[:span_len, :]
    for s in range(prompts):
        at = pl.ds(s * span_len, span_len)
        last = jnp.concatenate([last_a_ref[at, :], last_b_ref[at, :]], axis=1)
        total = total_ref[at, :] + arrived_ref[at, :]
        total += jnp.dot(last, last_weights, preferred_element_type=jnp.float32)
        keys = total[:, :inner]
        values = total[:, inner:].astype(jnp.bfloat16)
        keys = (keys * cosine + swap_halves(keys) * sine).astype(jnp.bfloat16)
        weighted = (keys.astype(jnp.float32) * decay).astype(jnp.bfloat16)
        full = lax.dot_general(
            weighted, values, (((0,), (0,)), ((), ())), preferred_element_type=jnp.float32
        )
        state = jnp.where(lane < HD, full[:HD], full[HD:]) * carried
        column = jnp.where(lane < HD, columns[:HD, s : s + 1], columns[HD:, s : s + 1])
        read = jnp.sum(state * column, axis=0, keepdims=True) * one
        for g in range(groups):
            out_ref[g, s * keep : (s + 1) * keep, :] = state[g * keep : (g + 1) * keep]
            out_ref[g, prompts * keep + s : prompts * keep + s + 1, :] = read


def span_states(prompts, groups, inner, place, *operands):
    keep = HD // groups
    whole = pl.BlockSpec(memory_space=pltpu.VMEM)
    return pl.pallas_call(
        state_kernel,
        in_specs=[pl.BlockSpec(memory_space=pltpu.SMEM)] + [whole] * len(operands),
        out_specs=[whole, whole],
        out_shape=[
            jax.ShapeDtypeStruct((groups, prompts * (keep + 1), inner), jnp.float32),
            jax.ShapeDtypeStruct((EXTRA, inner), jnp.float32),
        ],
        compiler_params=pltpu.CompilerParams(vmem_limit_bytes=8 * 1024 * 1024),
        name="span_states",
    )(place, *operands)


def finish_kernel(arrived_ref, own_ref, state_ref, read_ref):
    total = jnp.sum(arrived_ref[...], axis=0)
    prompts, heads, keep, _ = state_ref.shape
    for s in range(prompts):
        for h in range(heads):
            state_ref[s, h] = total[s * keep : (s + 1) * keep, h * HD : (h + 1) * HD].astype(
                jnp.bfloat16
            )
    raw = total[prompts * keep :] + own_ref[:prompts, :]
    lane = lax.broadcasted_iota(jnp.int32, raw.shape, 1)

    def per_head(values):
        result = jnp.zeros_like(values)
        for h in range(heads):
            here = lane // HD == h
            mean = jnp.sum(jnp.where(here, values, 0.0), axis=1, keepdims=True) / HD
            result = jnp.where(here, mean, result)
        return result

    centered = raw - per_head(raw)
    spread = per_head(centered * centered)
    read_ref[...] = (centered * lax.rsqrt(spread + EPS)).astype(jnp.bfloat16)


def finish(arrived, own_term, prompts, heads, keep):
    inner = own_term.shape[1]
    whole = pl.BlockSpec(memory_space=pltpu.VMEM)
    return pl.pallas_call(
        finish_kernel,
        in_specs=[whole, whole],
        out_specs=[whole, whole],
        out_shape=[
            jax.ShapeDtypeStruct((prompts, heads, keep, HD), jnp.bfloat16),
            jax.ShapeDtypeStruct((prompts, inner), jnp.bfloat16),
        ],
        compiler_params=pltpu.CompilerParams(vmem_limit_bytes=4 * 1024 * 1024),
        name="finish",
    )(arrived, own_term)


def tables(first_position, span_len, new_position, heads):
    quarter = HD // 2
    lane = jnp.arange(heads * HD, dtype=jnp.int32)
    inverse = 10000.0 ** (-(lane % quarter).astype(jnp.float32) / quarter)
    row = jnp.arange(span_len + 8, dtype=jnp.int32)
    position = jnp.where(row < span_len, first_position + row, new_position).astype(jnp.float32)
    angles = position[:, None] * inverse[None, :]
    key_scale = HD ** (-0.5)
    sign = jnp.where(lane % HD < quarter, -key_scale, key_scale)
    return jnp.cos(angles) * key_scale, jnp.sin(angles) * sign[None, :]


def body(tokens, new_token, query_weight, key_weight, value_weight, log_decay):
    prompts, span_len, width = tokens.shape
    heads = log_decay.shape[0]
    inner = heads * HD
    groups = lax.axis_size("sp")
    own_index = lax.axis_index("sp")
    tp_index = lax.axis_index("tp")
    planes = lax.axis_size("tp") // 2
    reach = planes // 2
    plane = tp_index // 2
    core = tp_index % 2
    rows = prompts * span_len
    place = jnp.stack([plane, core, own_index, jnp.int32(planes)]).astype(jnp.int32)

    partner = [(i, i ^ 1) for i in range(2 * planes)]
    onward = [
        (2 * z + c, 2 * ((z + (1 if c == 0 else -1)) % planes) + c)
        for z in range(planes)
        for c in range(2)
    ]

    across = [
        (2 * z + 1 - c, 2 * ((z + (1 if c == 0 else -1)) % planes) + c)
        for z in range(planes)
        for c in range(2)
    ]

    def sent(value, pairs):
        return lax.ppermute(value, "tp", pairs)

    tokens = tokens.reshape(rows, width)
    chain_a = sent(tokens, onward)
    chain_b = sent(tokens, across)
    fresh = new_token[:, 0]
    other_fresh = sent(new_token, partner)[:, 0]
    padding = jnp.zeros((EXTRA - prompts, width), new_token.dtype)
    new_pair = jnp.concatenate(
        [
            jnp.where(core == 0, fresh, other_fresh),
            padding,
            jnp.where(core == 0, other_fresh, fresh),
            padding,
        ],
        axis=0,
    )
    new_first = sent(new_pair, onward)
    a_list, b_list = [tokens, chain_a], [None, chain_b]
    new_list = [new_first]
    chain_a, first_position, log_decay = lax.optimization_barrier(
        (chain_a, own_index * span_len, log_decay)
    )
    a_list[1] = chain_a
    cosine, sine = tables(first_position, span_len, groups * span_len, heads)
    lane_decay = jnp.repeat(log_decay, HD)[None, :]
    new_first, cosine, sine, lane_decay = lax.optimization_barrier(
        (new_first, cosine, sine, lane_decay)
    )
    chain_b = jnp.concatenate([chain_b, new_first], axis=0)
    key_weight, value_weight, chain_b = lax.optimization_barrier(
        (key_weight, value_weight, chain_b)
    )
    main_weights = beside(key_weight, value_weight)
    other_weights = sent(main_weights, partner)
    b_list[0] = sent(tokens, partner)
    for _ in range(2, reach + 1):
        chain_a = sent(chain_a, onward)
        chain_b = sent(chain_b, onward)
        a_list.append(chain_a)
        b_list.append(chain_b)
        new_list.append(chain_b[rows:])
    sums = ()
    for offsets in ((1, 2), (0, 3, 4), (5, 6), (7,)):
        sums = ring_sums(
            offsets,
            span_len,
            place,
            main_weights,
            other_weights,
            [a_list[k] for k in offsets],
            [b_list[k] for k in offsets],
            sums,
        )
    own, other = sums

    arrived = sent(other, partner)
    mine_new = jnp.concatenate(new_list[:-1], axis=0)
    theirs_new = sent(mine_new, partner)

    messages, own_term = span_states(
        prompts,
        groups,
        inner,
        place,
        own,
        arrived,
        new_pair,
        mine_new,
        theirs_new,
        a_list[-1],
        b_list[-1],
        main_weights,
        query_weight,
        cosine,
        sine,
        lane_decay,
    )
    arrived = lax.all_to_all(messages, "sp", split_axis=0, concat_axis=0, tiled=True)
    return tuple(finish(arrived, own_term, prompts, heads, HD // groups))


def solution(mesh):
    return jax.shard_map(
        body,
        mesh=mesh,
        in_specs=(
            P(None, "sp", "tp"),
            P(None, None, "tp"),
            P(None, "tp"),
            P(None, "tp"),
            P(None, "tp"),
            P("tp"),
        ),
        out_specs=(P(None, "tp", "sp", None), P(None, "tp")),
        check_vma=False,
    )
```

```python
import functools

import jax
import jax.numpy as jnp
from jax import lax
from jax.experimental import pallas as pl
from jax.experimental.pallas import tpu as pltpu
from jax.sharding import PartitionSpec as P

HD = 64
EPS = 1e-05
EXTRA = 16


def swap_halves(values):
    lanes = values.shape[-1]
    lane = lax.broadcasted_iota(jnp.int32, values.shape, len(values.shape) - 1)
    quarter = HD // 2
    back = pltpu.roll(values, lanes - quarter, len(values.shape) - 1)
    ahead = pltpu.roll(values, quarter, len(values.shape) - 1)
    return jnp.where(lane % HD < quarter, back, ahead)


def beside_kernel(left_ref, right_ref, out_ref):
    width = left_ref.shape[1]
    out_ref[:, :width] = left_ref[...]
    out_ref[:, width:] = right_ref[...]


def beside(left, right):
    rows, width = left.shape
    whole = pl.BlockSpec(memory_space=pltpu.VMEM)
    return pl.pallas_call(
        beside_kernel,
        in_specs=[whole, whole],
        out_specs=whole,
        out_shape=jax.ShapeDtypeStruct((rows, 2 * width), left.dtype),
        compiler_params=pltpu.CompilerParams(vmem_limit_bytes=6 * 1024 * 1024),
        cost_estimate=pl.CostEstimate(flops=10**8, bytes_accessed=0, transcendentals=0),
        name="beside",
    )(left, right)


def row_block(place_ref, offset):
    planes = place_ref[3]
    toward = 1 - 2 * place_ref[1]
    return lax.rem(place_ref[0] - offset * toward + planes, planes)


def at_rows(block, width):
    return pl.ds(pl.multiple_of(block * width, width), width)


def stacked(place_ref, weight_ref, offsets, width):
    core = place_ref[1]
    blocks = []
    for offset in offsets:
        plane = row_block(place_ref, offset)
        blocks.append(weight_ref[at_rows(2 * plane + core, width), :])
        blocks.append(weight_ref[at_rows(2 * plane + 1 - core, width), :])
    return jnp.concatenate(blocks, axis=0)


def sums_kernel(offsets, span_len, has_before, place_ref, own_w_ref, other_w_ref, *refs):
    count = len(offsets)
    a_refs, b_refs, rest = refs[:count], refs[count : 2 * count], refs[2 * count :]
    before = rest[:2] if has_before else ()
    own_ref, other_ref, held, landed = rest[len(before) :]
    rows, width = a_refs[0].shape
    core = place_ref[1]
    hops = [i for i in range(count) if offsets[i] > 0]

    copies = []
    for j, i in enumerate(hops):
        plane = row_block(place_ref, offsets[i])
        for side, block in enumerate((2 * plane + core, 2 * plane + 1 - core)):
            slot = 2 * j + side
            copies.append(
                pltpu.make_async_copy(
                    other_w_ref.at[at_rows(block, width), :],
                    held.at[pl.ds(slot * width, width), :],
                    landed.at[slot],
                )
            )
    for copy in copies:
        copy.start()

    def summed(out_ref, earlier, which, weights_of):
        def step(s, carry):
            at = pl.ds(pl.multiple_of(s * span_len, span_len), span_len)
            pieces = []
            for i in which:
                pieces += [a_refs[i][at, :], b_refs[i][at, :]]
            both = jnp.concatenate(pieces, axis=1)
            part = jnp.dot(both, weights_of(), preferred_element_type=jnp.float32)
            if earlier is not None:
                part += earlier[at, :]
            out_ref[at, :] = part
            return carry

        lax.fori_loop(0, rows // span_len, step, 0)

    summed(
        own_ref,
        before[0] if before else None,
        list(range(count)),
        lambda: stacked(place_ref, own_w_ref, offsets, width),
    )
    for copy in copies:
        copy.wait()
    summed(other_ref, before[1] if before else None, hops, lambda: held[...])


def ring_sums(offsets, span_len, place, own_weights, other_weights, a_list, b_list, before):
    rows, width = a_list[0].shape
    inner = own_weights.shape[1]
    whole = pl.BlockSpec(memory_space=pltpu.VMEM)
    operands = [*a_list, *b_list, *before]
    blocks = 2 * sum(1 for offset in offsets if offset > 0)
    flops = 2 * rows * 2 * inner * 2 * width * len(offsets)
    return pl.pallas_call(
        functools.partial(sums_kernel, offsets, span_len, bool(before)),
        in_specs=[
            pl.BlockSpec(memory_space=pltpu.SMEM),
            whole,
            pl.BlockSpec(memory_space=pltpu.HBM),
        ]
        + [whole] * len(operands),
        out_specs=[whole, whole],
        out_shape=[jax.ShapeDtypeStruct((rows, inner), jnp.float32)] * 2,
        scratch_shapes=[
            pltpu.VMEM((blocks * width, inner), own_weights.dtype),
            pltpu.SemaphoreType.DMA((blocks,)),
        ],
        compiler_params=pltpu.CompilerParams(vmem_limit_bytes=6 * 1024 * 1024),
        cost_estimate=pl.CostEstimate(flops=flops, bytes_accessed=0, transcendentals=0),
        name="ring_sums",
    )(place, own_weights, other_weights, *operands)


def state_kernel(
    place_ref,
    rate_ref,
    total_ref,
    arrived_ref,
    here_new_ref,
    mine_new_ref,
    theirs_new_ref,
    last_a_ref,
    last_b_ref,
    main_ref,
    query_w_ref,
    cos_ref,
    sin_ref,
    out_ref,
    own_ref,
):
    rows, width = last_a_ref.shape
    inner = query_w_ref.shape[1]
    groups, out_rows, _ = out_ref.shape
    keep = HD // groups
    prompts = out_rows // (keep + 1)
    span_len = rows // prompts
    reach = mine_new_ref.shape[0] // (2 * EXTRA) + 1
    lane = lax.broadcasted_iota(jnp.int32, (HD, inner), 1)
    row_lane = lax.broadcasted_iota(jnp.int32, (1, inner), 1)
    lane_decay = jnp.full((1, inner), rate_ref[0], jnp.float32)
    for h in range(1, inner // HD):
        lane_decay = jnp.where(row_lane // HD == h, rate_ref[h], lane_decay)
    distance = ((groups - 1 - place_ref[2]) * span_len).astype(jnp.float32)
    carried = jnp.exp(lane_decay * distance)
    one = jnp.exp(lane_decay)
    to_end = lax.broadcasted_iota(jnp.int32, (span_len, inner), 0)
    decay = jnp.exp((span_len - 1 - to_end).astype(jnp.float32) * lane_decay)

    def pair(ref, start):
        return [ref[start : start + EXTRA, :], ref[start + EXTRA : start + 2 * EXTRA, :]]

    pieces = pair(here_new_ref, 0)
    order = [0]
    for k in range(1, reach):
        pieces += pair(mine_new_ref, (k - 1) * 2 * EXTRA)
        pieces += pair(theirs_new_ref, (k - 1) * 2 * EXTRA)
        order += [k, -k]
    pieces += pair(last_b_ref, rows)
    order.append(reach)
    entries = jnp.concatenate(pieces, axis=1)
    plane_rows = [at_rows(row_block(place_ref, k), 2 * width) for k in order]
    weights = jnp.concatenate(
        [jnp.concatenate([main_ref[at, :], query_w_ref[at, :]], axis=1) for at in plane_rows], axis=0
    )
    fresh = jnp.dot(entries, weights, preferred_element_type=jnp.float32)
    new_cos = cos_ref[span_len : span_len + 1, :]
    new_sin = sin_ref[span_len : span_len + 1, :]
    new_key = fresh[:, :inner]
    new_key = new_key * new_cos + swap_halves(new_key) * new_sin
    new_key = new_key.astype(jnp.bfloat16).astype(jnp.float32)
    new_value = fresh[:, inner : 2 * inner].astype(jnp.bfloat16).astype(jnp.float32)
    query = fresh[:, 2 * inner :]
    query = (query * new_cos + swap_halves(query) * new_sin) * (HD**0.5)
    query = query.astype(jnp.bfloat16).astype(jnp.float32)
    products = query * new_key
    new_lane = lax.broadcasted_iota(jnp.int32, products.shape, 1)
    score = jnp.zeros_like(products)
    for h in range(inner // HD):
        here = new_lane // HD == h
        score = jnp.where(
            here, jnp.sum(jnp.where(here, products, 0.0), axis=1, keepdims=True), score
        )
    own_ref[...] = score * new_value
    columns = jnp.transpose(query)

    last_weights = stacked(place_ref, main_ref, [reach], width)
    cosine = cos_ref[:span_len, :]
    sine = sin_ref[:span_len, :]
    for s in range(prompts):
        at = pl.ds(s * span_len, span_len)
        last = jnp.concatenate([last_a_ref[at, :], last_b_ref[at, :]], axis=1)
        total = total_ref[at, :] + arrived_ref[at, :]
        total += jnp.dot(last, last_weights, preferred_element_type=jnp.float32)
        keys = total[:, :inner]
        values = total[:, inner:].astype(jnp.bfloat16)
        keys = (keys * cosine + swap_halves(keys) * sine).astype(jnp.bfloat16)
        weighted = (keys.astype(jnp.float32) * decay).astype(jnp.bfloat16)
        full = lax.dot_general(
            weighted, values, (((0,), (0,)), ((), ())), preferred_element_type=jnp.float32
        )
        state = jnp.where(lane < HD, full[:HD], full[HD:]) * carried
        column = jnp.where(lane < HD, columns[:HD, s : s + 1], columns[HD:, s : s + 1])
        read = jnp.sum(state * column, axis=0, keepdims=True) * one
        for g in range(groups):
            out_ref[g, s * keep : (s + 1) * keep, :] = state[g * keep : (g + 1) * keep]
            out_ref[g, prompts * keep + s : prompts * keep + s + 1, :] = read


def span_states(prompts, groups, inner, place, *operands, decay):
    keep = HD // groups
    whole = pl.BlockSpec(memory_space=pltpu.VMEM)
    return pl.pallas_call(
        state_kernel,
        in_specs=[pl.BlockSpec(memory_space=pltpu.SMEM)] * 2 + [whole] * len(operands),
        out_specs=[whole, whole],
        out_shape=[
            jax.ShapeDtypeStruct((groups, prompts * (keep + 1), inner), jnp.float32),
            jax.ShapeDtypeStruct((EXTRA, inner), jnp.float32),
        ],
        compiler_params=pltpu.CompilerParams(vmem_limit_bytes=8 * 1024 * 1024),
        name="span_states",
    )(place, decay, *operands)


def finish_kernel(arrived_ref, own_ref, state_ref, read_ref):
    total = jnp.sum(arrived_ref[...], axis=0)
    prompts, heads, keep, _ = state_ref.shape
    for s in range(prompts):
        for h in range(heads):
            state_ref[s, h] = total[s * keep : (s + 1) * keep, h * HD : (h + 1) * HD].astype(
                jnp.bfloat16
            )
    raw = total[prompts * keep :] + own_ref[:prompts, :]
    lane = lax.broadcasted_iota(jnp.int32, raw.shape, 1)

    def per_head(values):
        result = jnp.zeros_like(values)
        for h in range(heads):
            here = lane // HD == h
            mean = jnp.sum(jnp.where(here, values, 0.0), axis=1, keepdims=True) / HD
            result = jnp.where(here, mean, result)
        return result

    centered = raw - per_head(raw)
    spread = per_head(centered * centered)
    read_ref[...] = (centered * lax.rsqrt(spread + EPS)).astype(jnp.bfloat16)


def finish(arrived, own_term, prompts, heads, keep):
    inner = own_term.shape[1]
    whole = pl.BlockSpec(memory_space=pltpu.VMEM)
    return pl.pallas_call(
        finish_kernel,
        in_specs=[whole, whole],
        out_specs=[whole, whole],
        out_shape=[
            jax.ShapeDtypeStruct((prompts, heads, keep, HD), jnp.bfloat16),
            jax.ShapeDtypeStruct((prompts, inner), jnp.bfloat16),
        ],
        compiler_params=pltpu.CompilerParams(vmem_limit_bytes=4 * 1024 * 1024),
        name="finish",
    )(arrived, own_term)


def tables(first_position, span_len, new_position, heads):
    quarter = HD // 2
    lane = jnp.arange(heads * HD, dtype=jnp.int32)
    inverse = 10000.0 ** (-(lane % quarter).astype(jnp.float32) / quarter)
    row = jnp.arange(span_len + 8, dtype=jnp.int32)
    position = jnp.where(row < span_len, first_position + row, new_position).astype(jnp.float32)
    angles = position[:, None] * inverse[None, :]
    key_scale = HD ** (-0.5)
    sign = jnp.where(lane % HD < quarter, -key_scale, key_scale)
    return jnp.cos(angles) * key_scale, jnp.sin(angles) * sign[None, :]


def body(tokens, new_token, query_weight, key_weight, value_weight, log_decay):
    prompts, span_len, width = tokens.shape
    heads = log_decay.shape[0]
    inner = heads * HD
    groups = lax.axis_size("sp")
    own_index = lax.axis_index("sp")
    tp_index = lax.axis_index("tp")
    planes = lax.axis_size("tp") // 2
    reach = planes // 2
    plane = tp_index // 2
    core = tp_index % 2
    rows = prompts * span_len
    place = jnp.stack([plane, core, own_index, jnp.int32(planes)]).astype(jnp.int32)

    partner = [(i, i ^ 1) for i in range(2 * planes)]
    onward = [
        (2 * z + c, 2 * ((z + (1 if c == 0 else -1)) % planes) + c)
        for z in range(planes)
        for c in range(2)
    ]

    across = [
        (2 * z + 1 - c, 2 * ((z + (1 if c == 0 else -1)) % planes) + c)
        for z in range(planes)
        for c in range(2)
    ]

    def sent(value, pairs):
        return lax.ppermute(value, "tp", pairs)

    tokens = tokens.reshape(rows, width)
    chain_a = sent(tokens, onward)
    chain_b = sent(tokens, across)
    fresh = new_token[:, 0]
    other_fresh = sent(new_token, partner)[:, 0]
    padding = jnp.zeros((EXTRA - prompts, width), new_token.dtype)
    new_pair = jnp.concatenate(
        [
            jnp.where(core == 0, fresh, other_fresh),
            padding,
            jnp.where(core == 0, other_fresh, fresh),
            padding,
        ],
        axis=0,
    )
    new_first = sent(new_pair, onward)
    a_list, b_list = [tokens, chain_a], [None, chain_b]
    new_list = [new_first]
    chain_a, first_position = lax.optimization_barrier((chain_a, own_index * span_len))
    a_list[1] = chain_a
    cosine, sine = tables(first_position, span_len, groups * span_len, heads)
    new_first, cosine, sine = lax.optimization_barrier((new_first, cosine, sine))
    chain_b = jnp.concatenate([chain_b, new_first], axis=0)
    key_weight, value_weight, chain_b = lax.optimization_barrier(
        (key_weight, value_weight, chain_b)
    )
    main_weights = beside(key_weight, value_weight)
    other_weights = sent(main_weights, partner)
    b_list[0] = sent(tokens, partner)
    for _ in range(2, reach + 1):
        chain_a = sent(chain_a, onward)
        chain_b = sent(chain_b, onward)
        a_list.append(chain_a)
        b_list.append(chain_b)
        new_list.append(chain_b[rows:])
    sums = ()
    for offsets in ((1, 2), (0, 3, 4), (5, 6), (7,)):
        sums = ring_sums(
            offsets,
            span_len,
            place,
            main_weights,
            other_weights,
            [a_list[k] for k in offsets],
            [b_list[k] for k in offsets],
            sums,
        )
    own, other = sums

    arrived = sent(other, partner)
    mine_new = jnp.concatenate(new_list[:-1], axis=0)
    theirs_new = sent(mine_new, partner)

    messages, own_term = span_states(
        prompts,
        groups,
        inner,
        place,
        own,
        arrived,
        new_pair,
        mine_new,
        theirs_new,
        a_list[-1],
        b_list[-1],
        main_weights,
        query_weight,
        cosine,
        sine,
        decay=log_decay,
    )
    arrived = lax.all_to_all(messages, "sp", split_axis=0, concat_axis=0, tiled=True)
    return tuple(finish(arrived, own_term, prompts, heads, HD // groups))


def solution(mesh):
    return jax.shard_map(
        body,
        mesh=mesh,
        in_specs=(
            P(None, "sp", "tp"),
            P(None, None, "tp"),
            P(None, "tp"),
            P(None, "tp"),
            P(None, "tp"),
            P("tp"),
        ),
        out_specs=(P(None, "tp", "sp", None), P(None, "tp")),
        check_vma=False,
    )
```

```python
import functools

import jax
import jax.numpy as jnp
from jax import lax
from jax.experimental import pallas as pl
from jax.experimental.pallas import tpu as pltpu
from jax.sharding import PartitionSpec as P

HD = 64
EPS = 1e-05
EXTRA = 16


def swap_halves(values):
    lanes = values.shape[-1]
    lane = lax.broadcasted_iota(jnp.int32, values.shape, len(values.shape) - 1)
    quarter = HD // 2
    back = pltpu.roll(values, lanes - quarter, len(values.shape) - 1)
    ahead = pltpu.roll(values, quarter, len(values.shape) - 1)
    return jnp.where(lane % HD < quarter, back, ahead)


def beside_kernel(left_ref, right_ref, out_ref):
    width = left_ref.shape[1]
    out_ref[:, :width] = left_ref[...]
    out_ref[:, width:] = right_ref[...]


def beside(left, right):
    rows, width = left.shape
    whole = pl.BlockSpec(memory_space=pltpu.VMEM)
    return pl.pallas_call(
        beside_kernel,
        in_specs=[whole, whole],
        out_specs=whole,
        out_shape=jax.ShapeDtypeStruct((rows, 2 * width), left.dtype),
        compiler_params=pltpu.CompilerParams(vmem_limit_bytes=6 * 1024 * 1024),
        cost_estimate=pl.CostEstimate(flops=10**8, bytes_accessed=0, transcendentals=0),
        name="beside",
    )(left, right)


def row_block(place_ref, offset):
    planes = place_ref[3]
    toward = 1 - 2 * place_ref[1]
    return lax.rem(place_ref[0] - offset * toward + planes, planes)


def at_rows(block, width):
    return pl.ds(pl.multiple_of(block * width, width), width)


def stacked(place_ref, weight_ref, offsets, width):
    core = place_ref[1]
    blocks = []
    for offset in offsets:
        plane = row_block(place_ref, offset)
        blocks.append(weight_ref[at_rows(2 * plane + core, width), :])
        blocks.append(weight_ref[at_rows(2 * plane + 1 - core, width), :])
    return jnp.concatenate(blocks, axis=0)


def sums_kernel(offsets, span_len, has_before, place_ref, own_w_ref, other_w_ref, *refs):
    count = len(offsets)
    a_refs, b_refs, rest = refs[:count], refs[count : 2 * count], refs[2 * count :]
    before = rest[:2] if has_before else ()
    own_ref, other_ref, held, landed = rest[len(before) :]
    rows, width = a_refs[0].shape
    core = place_ref[1]
    hops = [i for i in range(count) if offsets[i] > 0]

    copies = []
    for j, i in enumerate(hops):
        plane = row_block(place_ref, offsets[i])
        for side, block in enumerate((2 * plane + core, 2 * plane + 1 - core)):
            slot = 2 * j + side
            copies.append(
                pltpu.make_async_copy(
                    other_w_ref.at[at_rows(block, width), :],
                    held.at[pl.ds(slot * width, width), :],
                    landed.at[slot],
                )
            )
    for copy in copies:
        copy.start()

    def summed(out_ref, earlier, which, weights_of):
        def step(s, carry):
            at = pl.ds(pl.multiple_of(s * span_len, span_len), span_len)
            pieces = []
            for i in which:
                pieces += [a_refs[i][at, :], b_refs[i][at, :]]
            both = jnp.concatenate(pieces, axis=1)
            part = jnp.dot(both, weights_of(), preferred_element_type=jnp.float32)
            if earlier is not None:
                part += earlier[at, :]
            out_ref[at, :] = part
            return carry

        lax.fori_loop(0, rows // span_len, step, 0)

    summed(
        own_ref,
        before[0] if before else None,
        list(range(count)),
        lambda: stacked(place_ref, own_w_ref, offsets, width),
    )
    for copy in copies:
        copy.wait()
    summed(other_ref, before[1] if before else None, hops, lambda: held[...])


def ring_sums(offsets, span_len, place, own_weights, other_weights, a_list, b_list, before):
    rows, width = a_list[0].shape
    inner = own_weights.shape[1]
    whole = pl.BlockSpec(memory_space=pltpu.VMEM)
    operands = [*a_list, *b_list, *before]
    blocks = 2 * sum(1 for offset in offsets if offset > 0)
    flops = 2 * rows * 2 * inner * 2 * width * len(offsets)
    return pl.pallas_call(
        functools.partial(sums_kernel, offsets, span_len, bool(before)),
        in_specs=[
            pl.BlockSpec(memory_space=pltpu.SMEM),
            whole,
            pl.BlockSpec(memory_space=pltpu.HBM),
        ]
        + [whole] * len(operands),
        out_specs=[whole, whole],
        out_shape=[jax.ShapeDtypeStruct((rows, inner), jnp.float32)] * 2,
        scratch_shapes=[
            pltpu.VMEM((blocks * width, inner), own_weights.dtype),
            pltpu.SemaphoreType.DMA((blocks,)),
        ],
        compiler_params=pltpu.CompilerParams(vmem_limit_bytes=6 * 1024 * 1024),
        cost_estimate=pl.CostEstimate(flops=flops, bytes_accessed=0, transcendentals=0),
        name="ring_sums",
    )(place, own_weights, other_weights, *operands)


def state_kernel(
    place_ref,
    rate_ref,
    total_ref,
    arrived_ref,
    here_new_ref,
    mine_new_ref,
    theirs_new_ref,
    tail_a_ref,
    tail_b_ref,
    passed_a_ref,
    passed_b_ref,
    main_ref,
    query_w_ref,
    cos_ref,
    sin_ref,
    out_ref,
    own_ref,
):
    rows, width = tail_a_ref.shape
    inner = query_w_ref.shape[1]
    groups, out_rows, _ = out_ref.shape
    keep = HD // groups
    prompts = out_rows // (keep + 1)
    span_len = rows // prompts
    reach = mine_new_ref.shape[0] // (2 * EXTRA) + 1
    lane = lax.broadcasted_iota(jnp.int32, (HD, inner), 1)
    row_lane = lax.broadcasted_iota(jnp.int32, (1, inner), 1)
    lane_decay = jnp.full((1, inner), rate_ref[0], jnp.float32)
    for h in range(1, inner // HD):
        lane_decay = jnp.where(row_lane // HD == h, rate_ref[h], lane_decay)
    distance = ((groups - 1 - place_ref[2]) * span_len).astype(jnp.float32)
    carried = jnp.exp(lane_decay * distance)
    one = jnp.exp(lane_decay)
    to_end = lax.broadcasted_iota(jnp.int32, (span_len, inner), 0)
    decay = jnp.exp((span_len - 1 - to_end).astype(jnp.float32) * lane_decay)

    def pair(ref, start):
        return [ref[start : start + EXTRA, :], ref[start + EXTRA : start + 2 * EXTRA, :]]

    pieces = pair(here_new_ref, 0)
    order = [0]
    for k in range(1, reach):
        pieces += pair(mine_new_ref, (k - 1) * 2 * EXTRA)
        pieces += pair(theirs_new_ref, (k - 1) * 2 * EXTRA)
        order += [k, -k]
    pieces += [x + y for x, y in zip(pair(tail_b_ref, rows), pair(passed_b_ref, rows))]
    order.append(reach)
    entries = jnp.concatenate(pieces, axis=1)
    plane_rows = [at_rows(row_block(place_ref, k), 2 * width) for k in order]
    weights = jnp.concatenate(
        [jnp.concatenate([main_ref[at, :], query_w_ref[at, :]], axis=1) for at in plane_rows], axis=0
    )
    fresh = jnp.dot(entries, weights, preferred_element_type=jnp.float32)
    new_cos = cos_ref[span_len : span_len + 1, :]
    new_sin = sin_ref[span_len : span_len + 1, :]
    new_key = fresh[:, :inner]
    new_key = new_key * new_cos + swap_halves(new_key) * new_sin
    new_key = new_key.astype(jnp.bfloat16).astype(jnp.float32)
    new_value = fresh[:, inner : 2 * inner].astype(jnp.bfloat16).astype(jnp.float32)
    query = fresh[:, 2 * inner :]
    query = (query * new_cos + swap_halves(query) * new_sin) * (HD**0.5)
    query = query.astype(jnp.bfloat16).astype(jnp.float32)
    products = query * new_key
    new_lane = lax.broadcasted_iota(jnp.int32, products.shape, 1)
    score = jnp.zeros_like(products)
    for h in range(inner // HD):
        here = new_lane // HD == h
        score = jnp.where(
            here, jnp.sum(jnp.where(here, products, 0.0), axis=1, keepdims=True), score
        )
    own_ref[...] = score * new_value
    columns = jnp.transpose(query)

    last_weights = main_ref[at_rows(row_block(place_ref, reach), 2 * width), :]
    cosine = cos_ref[:span_len, :]
    sine = sin_ref[:span_len, :]
    for s in range(prompts):
        at = pl.ds(s * span_len, span_len)
        last = jnp.concatenate(
            [
                tail_b_ref[at, :] + passed_b_ref[at, :],
                tail_a_ref[at, :] + passed_a_ref[at, :],
            ],
            axis=1,
        )
        total = total_ref[at, :] + arrived_ref[at, :]
        total += jnp.dot(last, last_weights, preferred_element_type=jnp.float32)
        keys = total[:, :inner]
        values = total[:, inner:].astype(jnp.bfloat16)
        keys = (keys * cosine + swap_halves(keys) * sine).astype(jnp.bfloat16)
        weighted = (keys.astype(jnp.float32) * decay).astype(jnp.bfloat16)
        full = lax.dot_general(
            weighted, values, (((0,), (0,)), ((), ())), preferred_element_type=jnp.float32
        )
        state = jnp.where(lane < HD, full[:HD], full[HD:]) * carried
        column = jnp.where(lane < HD, columns[:HD, s : s + 1], columns[HD:, s : s + 1])
        read = jnp.sum(state * column, axis=0, keepdims=True) * one
        for g in range(groups):
            out_ref[g, s * keep : (s + 1) * keep, :] = state[g * keep : (g + 1) * keep]
            out_ref[g, prompts * keep + s : prompts * keep + s + 1, :] = read


def span_states(prompts, groups, inner, place, *operands, decay):
    keep = HD // groups
    whole = pl.BlockSpec(memory_space=pltpu.VMEM)
    return pl.pallas_call(
        state_kernel,
        in_specs=[pl.BlockSpec(memory_space=pltpu.SMEM)] * 2 + [whole] * len(operands),
        out_specs=[whole, whole],
        out_shape=[
            jax.ShapeDtypeStruct((groups, prompts * (keep + 1), inner), jnp.float32),
            jax.ShapeDtypeStruct((EXTRA, inner), jnp.float32),
        ],
        compiler_params=pltpu.CompilerParams(vmem_limit_bytes=8 * 1024 * 1024),
        name="span_states",
    )(place, decay, *operands)


def finish_kernel(arrived_ref, own_ref, state_ref, read_ref):
    total = jnp.sum(arrived_ref[...], axis=0)
    prompts, heads, keep, _ = state_ref.shape
    for s in range(prompts):
        for h in range(heads):
            state_ref[s, h] = total[s * keep : (s + 1) * keep, h * HD : (h + 1) * HD].astype(
                jnp.bfloat16
            )
    raw = total[prompts * keep :] + own_ref[:prompts, :]
    lane = lax.broadcasted_iota(jnp.int32, raw.shape, 1)

    def per_head(values):
        result = jnp.zeros_like(values)
        for h in range(heads):
            here = lane // HD == h
            mean = jnp.sum(jnp.where(here, values, 0.0), axis=1, keepdims=True) / HD
            result = jnp.where(here, mean, result)
        return result

    centered = raw - per_head(raw)
    spread = per_head(centered * centered)
    read_ref[...] = (centered * lax.rsqrt(spread + EPS)).astype(jnp.bfloat16)


def finish(arrived, own_term, prompts, heads, keep):
    inner = own_term.shape[1]
    whole = pl.BlockSpec(memory_space=pltpu.VMEM)
    return pl.pallas_call(
        finish_kernel,
        in_specs=[whole, whole],
        out_specs=[whole, whole],
        out_shape=[
            jax.ShapeDtypeStruct((prompts, heads, keep, HD), jnp.bfloat16),
            jax.ShapeDtypeStruct((prompts, inner), jnp.bfloat16),
        ],
        compiler_params=pltpu.CompilerParams(vmem_limit_bytes=4 * 1024 * 1024),
        name="finish",
    )(arrived, own_term)


def tables(first_position, span_len, new_position, heads):
    quarter = HD // 2
    lane = jnp.arange(heads * HD, dtype=jnp.int32)
    inverse = 10000.0 ** (-(lane % quarter).astype(jnp.float32) / quarter)
    row = jnp.arange(span_len + 8, dtype=jnp.int32)
    position = jnp.where(row < span_len, first_position + row, new_position).astype(jnp.float32)
    angles = position[:, None] * inverse[None, :]
    key_scale = HD ** (-0.5)
    sign = jnp.where(lane % HD < quarter, -key_scale, key_scale)
    return jnp.cos(angles) * key_scale, jnp.sin(angles) * sign[None, :]


def body(tokens, new_token, query_weight, key_weight, value_weight, log_decay):
    prompts, span_len, width = tokens.shape
    heads = log_decay.shape[0]
    inner = heads * HD
    groups = lax.axis_size("sp")
    own_index = lax.axis_index("sp")
    tp_index = lax.axis_index("tp")
    planes = lax.axis_size("tp") // 2
    reach = planes // 2
    plane = tp_index // 2
    core = tp_index % 2
    rows = prompts * span_len
    place = jnp.stack([plane, core, own_index, jnp.int32(planes)]).astype(jnp.int32)

    partner = [(i, i ^ 1) for i in range(2 * planes)]
    onward = [
        (2 * z + c, 2 * ((z + (1 if c == 0 else -1)) % planes) + c)
        for z in range(planes)
        for c in range(2)
    ]

    across = [
        (2 * z + 1 - c, 2 * ((z + (1 if c == 0 else -1)) % planes) + c)
        for z in range(planes)
        for c in range(2)
    ]

    def sent(value, pairs):
        return lax.ppermute(value, "tp", pairs)

    tokens = tokens.reshape(rows, width)
    chain_a = sent(tokens, onward)
    chain_b = sent(tokens, across)
    fresh = new_token[:, 0]
    other_fresh = sent(new_token, partner)[:, 0]
    padding = jnp.zeros((EXTRA - prompts, width), new_token.dtype)
    new_pair = jnp.concatenate(
        [
            jnp.where(core == 0, fresh, other_fresh),
            padding,
            jnp.where(core == 0, other_fresh, fresh),
            padding,
        ],
        axis=0,
    )
    new_first = sent(new_pair, onward)
    a_list, b_list = [tokens, chain_a], [None, chain_b]
    new_list = [new_first]
    chain_a, first_position = lax.optimization_barrier((chain_a, own_index * span_len))
    a_list[1] = chain_a
    cosine, sine = tables(first_position, span_len, groups * span_len, heads)
    new_first, cosine, sine = lax.optimization_barrier((new_first, cosine, sine))
    chain_b = jnp.concatenate([chain_b, new_first], axis=0)
    key_weight, value_weight, chain_b = lax.optimization_barrier(
        (key_weight, value_weight, chain_b)
    )
    main_weights = beside(key_weight, value_weight)
    other_weights = sent(main_weights, partner)
    b_list[0] = sent(tokens, partner)
    for _ in range(2, reach):
        chain_a = sent(chain_a, onward)
        chain_b = sent(chain_b, onward)
        a_list.append(chain_a)
        b_list.append(chain_b)
        new_list.append(chain_b[rows:])
    down = [(2 * z + 1, 2 * ((z - 1) % planes) + 1) for z in range(planes)]
    inward = [(2 * z + 1, 2 * z) for z in range(planes)]
    tail_a = sent(chain_a, down)
    tail_b = sent(chain_b, down)
    sums = ()
    for offsets in ((1, 2), (0, 3, 4), (5, 6), (7,)):
        sums = ring_sums(
            offsets,
            span_len,
            place,
            main_weights,
            other_weights,
            [a_list[k] for k in offsets],
            [b_list[k] for k in offsets],
            sums,
        )
    own, other = sums

    arrived = sent(other, partner)
    mine_new = jnp.concatenate(new_list, axis=0)
    theirs_new = sent(mine_new, partner)
    passed_a = sent(tail_a, inward)
    passed_b = sent(tail_b, inward)

    messages, own_term = span_states(
        prompts,
        groups,
        inner,
        place,
        own,
        arrived,
        new_pair,
        mine_new,
        theirs_new,
        tail_a,
        tail_b,
        passed_a,
        passed_b,
        main_weights,
        query_weight,
        cosine,
        sine,
        decay=log_decay,
    )
    arrived = lax.all_to_all(messages, "sp", split_axis=0, concat_axis=0, tiled=True)
    return tuple(finish(arrived, own_term, prompts, heads, HD // groups))


def solution(mesh):
    return jax.shard_map(
        body,
        mesh=mesh,
        in_specs=(
            P(None, "sp", "tp"),
            P(None, None, "tp"),
            P(None, "tp"),
            P(None, "tp"),
            P(None, "tp"),
            P("tp"),
        ),
        out_specs=(P(None, "tp", "sp", None), P(None, "tp")),
        check_vma=False,
    )
```

```python
import functools

import jax
import jax.numpy as jnp
from jax import lax
from jax.experimental import pallas as pl
from jax.experimental.pallas import tpu as pltpu
from jax.sharding import PartitionSpec as P

HD = 64
EPS = 1e-05
EXTRA = 16


def swap_halves(values):
    lanes = values.shape[-1]
    lane = lax.broadcasted_iota(jnp.int32, values.shape, len(values.shape) - 1)
    quarter = HD // 2
    back = pltpu.roll(values, lanes - quarter, len(values.shape) - 1)
    ahead = pltpu.roll(values, quarter, len(values.shape) - 1)
    return jnp.where(lane % HD < quarter, back, ahead)


def beside_kernel(left_ref, right_ref, out_ref):
    width = left_ref.shape[1]
    out_ref[:, :width] = left_ref[...]
    out_ref[:, width:] = right_ref[...]


def beside(left, right):
    rows, width = left.shape
    whole = pl.BlockSpec(memory_space=pltpu.VMEM)
    return pl.pallas_call(
        beside_kernel,
        in_specs=[whole, whole],
        out_specs=whole,
        out_shape=jax.ShapeDtypeStruct((rows, 2 * width), left.dtype),
        compiler_params=pltpu.CompilerParams(vmem_limit_bytes=6 * 1024 * 1024),
        cost_estimate=pl.CostEstimate(flops=10**8, bytes_accessed=0, transcendentals=0),
        name="beside",
    )(left, right)


def row_block(place_ref, offset):
    planes = place_ref[3]
    toward = 1 - 2 * place_ref[1]
    return lax.rem(place_ref[0] - offset * toward + planes, planes)


def at_rows(block, width):
    return pl.ds(pl.multiple_of(block * width, width), width)


def stacked(place_ref, weight_ref, offsets, width):
    core = place_ref[1]
    blocks = []
    for offset in offsets:
        plane = row_block(place_ref, offset)
        blocks.append(weight_ref[at_rows(2 * plane + core, width), :])
        blocks.append(weight_ref[at_rows(2 * plane + 1 - core, width), :])
    return jnp.concatenate(blocks, axis=0)


def sums_kernel(offsets, span_len, has_before, place_ref, own_w_ref, other_w_ref, *refs):
    count = len(offsets)
    a_refs, b_refs, rest = refs[:count], refs[count : 2 * count], refs[2 * count :]
    before, rest = (rest[:2], rest[2:]) if has_before else ((), rest)
    tails, (own_ref, other_ref, held, landed) = rest[:-4], rest[-4:]
    rows, width = a_refs[0].shape
    for i, tail_ref in enumerate(tails):
        other_ref[rows:, i * width : (i + 1) * width] = tail_ref[...].astype(jnp.float32)
    core = place_ref[1]
    hops = [i for i in range(count) if offsets[i] > 0]

    copies = []
    for j, i in enumerate(hops):
        plane = row_block(place_ref, offsets[i])
        for side, block in enumerate((2 * plane + core, 2 * plane + 1 - core)):
            slot = 2 * j + side
            copies.append(
                pltpu.make_async_copy(
                    other_w_ref.at[at_rows(block, width), :],
                    held.at[pl.ds(slot * width, width), :],
                    landed.at[slot],
                )
            )
    for copy in copies:
        copy.start()

    def summed(out_ref, earlier, which, weights_of):
        def step(s, carry):
            at = pl.ds(pl.multiple_of(s * span_len, span_len), span_len)
            pieces = []
            for i in which:
                pieces += [a_refs[i][at, :], b_refs[i][at, :]]
            both = jnp.concatenate(pieces, axis=1)
            part = jnp.dot(both, weights_of(), preferred_element_type=jnp.float32)
            if earlier is not None:
                part += earlier[at, :]
            out_ref[at, :] = part
            return carry

        lax.fori_loop(0, rows // span_len, step, 0)

    summed(
        own_ref,
        before[0] if before else None,
        list(range(count)),
        lambda: stacked(place_ref, own_w_ref, offsets, width),
    )
    for copy in copies:
        copy.wait()
    summed(other_ref, before[1] if before else None, hops, lambda: held[...])


def ring_sums(
    offsets, span_len, place, own_weights, other_weights, a_list, b_list, before, tails=()
):
    rows, width = a_list[0].shape
    inner = own_weights.shape[1]
    whole = pl.BlockSpec(memory_space=pltpu.VMEM)
    operands = [*a_list, *b_list, *before, *tails]
    more = tails[0].shape[0] if tails else 0
    blocks = 2 * sum(1 for offset in offsets if offset > 0)
    flops = 2 * rows * 2 * inner * 2 * width * len(offsets)
    return pl.pallas_call(
        functools.partial(sums_kernel, offsets, span_len, bool(before)),
        in_specs=[
            pl.BlockSpec(memory_space=pltpu.SMEM),
            whole,
            pl.BlockSpec(memory_space=pltpu.HBM),
        ]
        + [whole] * len(operands),
        out_specs=[whole, whole],
        out_shape=[
            jax.ShapeDtypeStruct((rows, inner), jnp.float32),
            jax.ShapeDtypeStruct((rows + more, inner), jnp.float32),
        ],
        scratch_shapes=[
            pltpu.VMEM((blocks * width, inner), own_weights.dtype),
            pltpu.SemaphoreType.DMA((blocks,)),
        ],
        compiler_params=pltpu.CompilerParams(vmem_limit_bytes=6 * 1024 * 1024),
        cost_estimate=pl.CostEstimate(flops=flops, bytes_accessed=0, transcendentals=0),
        name="ring_sums",
    )(place, own_weights, other_weights, *operands)


def state_kernel(
    place_ref,
    rate_ref,
    total_ref,
    arrived_ref,
    here_new_ref,
    mine_new_ref,
    near_new_ref,
    theirs_new_ref,
    far_new_ref,
    last_up_ref,
    last_down_ref,
    last_b_ref,
    passed_a_ref,
    main_ref,
    query_w_ref,
    cos_ref,
    sin_ref,
    out_ref,
    own_ref,
):
    rows, width = last_up_ref.shape
    inner = query_w_ref.shape[1]
    groups, out_rows, _ = out_ref.shape
    keep = HD // groups
    prompts = out_rows // (keep + 1)
    span_len = rows // prompts
    swapped = mine_new_ref.shape[0] // (2 * EXTRA)
    reach = swapped + near_new_ref.shape[0] // (2 * EXTRA) + 1
    lane = lax.broadcasted_iota(jnp.int32, (HD, inner), 1)
    row_lane = lax.broadcasted_iota(jnp.int32, (1, inner), 1)
    lane_decay = jnp.full((1, inner), rate_ref[0], jnp.float32)
    for h in range(1, inner // HD):
        lane_decay = jnp.where(row_lane // HD == h, rate_ref[h], lane_decay)
    distance = ((groups - 1 - place_ref[2]) * span_len).astype(jnp.float32)
    carried = jnp.exp(lane_decay * distance)
    one = jnp.exp(lane_decay)
    to_end = lax.broadcasted_iota(jnp.int32, (span_len, inner), 0)
    decay = jnp.exp((span_len - 1 - to_end).astype(jnp.float32) * lane_decay)

    def pair(ref, start):
        return [ref[start : start + EXTRA, :], ref[start + EXTRA : start + 2 * EXTRA, :]]

    pieces = pair(here_new_ref, 0)
    order = [0]
    for k in range(1, swapped + 1):
        pieces += pair(mine_new_ref, (k - 1) * 2 * EXTRA)
        pieces += pair(theirs_new_ref, (k - 1) * 2 * EXTRA)
        order += [k, -k]
    late = arrived_ref[rows:, :].astype(jnp.bfloat16)
    for k in range(swapped + 1, reach):
        i = k - swapped - 1
        pieces += pair(near_new_ref, i * 2 * EXTRA)
        theirs = late[:, i * width : (i + 1) * width]
        pieces += [theirs[:EXTRA], theirs[EXTRA:]]
        order += [k, -k]
    pieces += pair(far_new_ref, 0)
    order.append(reach)
    entries = jnp.concatenate(pieces, axis=1)
    plane_rows = [at_rows(row_block(place_ref, k), 2 * width) for k in order]
    weights = jnp.concatenate(
        [jnp.concatenate([main_ref[at, :], query_w_ref[at, :]], axis=1) for at in plane_rows], axis=0
    )
    fresh = jnp.dot(entries, weights, preferred_element_type=jnp.float32)
    new_cos = cos_ref[span_len : span_len + 1, :]
    new_sin = sin_ref[span_len : span_len + 1, :]
    new_key = fresh[:, :inner]
    new_key = new_key * new_cos + swap_halves(new_key) * new_sin
    new_key = new_key.astype(jnp.bfloat16).astype(jnp.float32)
    new_value = fresh[:, inner : 2 * inner].astype(jnp.bfloat16).astype(jnp.float32)
    query = fresh[:, 2 * inner :]
    query = (query * new_cos + swap_halves(query) * new_sin) * (HD**0.5)
    query = query.astype(jnp.bfloat16).astype(jnp.float32)
    products = query * new_key
    new_lane = lax.broadcasted_iota(jnp.int32, products.shape, 1)
    score = jnp.zeros_like(products)
    for h in range(inner // HD):
        here = new_lane // HD == h
        score = jnp.where(
            here, jnp.sum(jnp.where(here, products, 0.0), axis=1, keepdims=True), score
        )
    own_ref[...] = score * new_value
    columns = jnp.transpose(query)

    last_weights = stacked(place_ref, main_ref, [reach], width)
    cosine = cos_ref[:span_len, :]
    sine = sin_ref[:span_len, :]
    for s in range(prompts):
        at = pl.ds(s * span_len, span_len)
        other = last_b_ref[at, :] + passed_a_ref[at, :]
        mine = last_up_ref[at, :] + last_down_ref[at, :]
        last = jnp.concatenate([mine, other], axis=1)
        total = total_ref[at, :] + arrived_ref[at, :]
        total += jnp.dot(last, last_weights, preferred_element_type=jnp.float32)
        keys = total[:, :inner]
        values = total[:, inner:].astype(jnp.bfloat16)
        keys = (keys * cosine + swap_halves(keys) * sine).astype(jnp.bfloat16)
        weighted = (keys.astype(jnp.float32) * decay).astype(jnp.bfloat16)
        full = lax.dot_general(
            weighted, values, (((0,), (0,)), ((), ())), preferred_element_type=jnp.float32
        )
        state = jnp.where(lane < HD, full[:HD], full[HD:]) * carried
        column = jnp.where(lane < HD, columns[:HD, s : s + 1], columns[HD:, s : s + 1])
        read = jnp.sum(state * column, axis=0, keepdims=True) * one
        for g in range(groups):
            out_ref[g, s * keep : (s + 1) * keep, :] = state[g * keep : (g + 1) * keep]
            out_ref[g, prompts * keep + s : prompts * keep + s + 1, :] = read


def span_states(prompts, groups, inner, place, *operands, decay):
    keep = HD // groups
    whole = pl.BlockSpec(memory_space=pltpu.VMEM)
    return pl.pallas_call(
        state_kernel,
        in_specs=[pl.BlockSpec(memory_space=pltpu.SMEM)] * 2 + [whole] * len(operands),
        out_specs=[whole, whole],
        out_shape=[
            jax.ShapeDtypeStruct((groups, prompts * (keep + 1), inner), jnp.float32),
            jax.ShapeDtypeStruct((EXTRA, inner), jnp.float32),
        ],
        compiler_params=pltpu.CompilerParams(vmem_limit_bytes=8 * 1024 * 1024),
        name="span_states",
    )(place, decay, *operands)


def finish_kernel(arrived_ref, own_ref, state_ref, read_ref):
    total = jnp.sum(arrived_ref[...], axis=0)
    prompts, heads, keep, _ = state_ref.shape
    for s in range(prompts):
        for h in range(heads):
            state_ref[s, h] = total[s * keep : (s + 1) * keep, h * HD : (h + 1) * HD].astype(
                jnp.bfloat16
            )
    raw = total[prompts * keep :] + own_ref[:prompts, :]
    lane = lax.broadcasted_iota(jnp.int32, raw.shape, 1)

    def per_head(values):
        result = jnp.zeros_like(values)
        for h in range(heads):
            here = lane // HD == h
            mean = jnp.sum(jnp.where(here, values, 0.0), axis=1, keepdims=True) / HD
            result = jnp.where(here, mean, result)
        return result

    centered = raw - per_head(raw)
    spread = per_head(centered * centered)
    read_ref[...] = (centered * lax.rsqrt(spread + EPS)).astype(jnp.bfloat16)


def finish(arrived, own_term, prompts, heads, keep):
    inner = own_term.shape[1]
    whole = pl.BlockSpec(memory_space=pltpu.VMEM)
    return pl.pallas_call(
        finish_kernel,
        in_specs=[whole, whole],
        out_specs=[whole, whole],
        out_shape=[
            jax.ShapeDtypeStruct((prompts, heads, keep, HD), jnp.bfloat16),
            jax.ShapeDtypeStruct((prompts, inner), jnp.bfloat16),
        ],
        compiler_params=pltpu.CompilerParams(vmem_limit_bytes=4 * 1024 * 1024),
        name="finish",
    )(arrived, own_term)


def tables(first_position, span_len, new_position, heads):
    quarter = HD // 2
    lane = jnp.arange(heads * HD, dtype=jnp.int32)
    inverse = 10000.0 ** (-(lane % quarter).astype(jnp.float32) / quarter)
    row = jnp.arange(span_len + 8, dtype=jnp.int32)
    position = jnp.where(row < span_len, first_position + row, new_position).astype(jnp.float32)
    angles = position[:, None] * inverse[None, :]
    key_scale = HD ** (-0.5)
    sign = jnp.where(lane % HD < quarter, -key_scale, key_scale)
    return jnp.cos(angles) * key_scale, jnp.sin(angles) * sign[None, :]


def body(tokens, new_token, query_weight, key_weight, value_weight, log_decay):
    prompts, span_len, width = tokens.shape
    heads = log_decay.shape[0]
    inner = heads * HD
    groups = lax.axis_size("sp")
    own_index = lax.axis_index("sp")
    tp_index = lax.axis_index("tp")
    planes = lax.axis_size("tp") // 2
    reach = planes // 2
    plane = tp_index // 2
    core = tp_index % 2
    rows = prompts * span_len
    place = jnp.stack([plane, core, own_index, jnp.int32(planes)]).astype(jnp.int32)

    partner = [(i, i ^ 1) for i in range(2 * planes)]
    onward = [
        (2 * z + c, 2 * ((z + (1 if c == 0 else -1)) % planes) + c)
        for z in range(planes)
        for c in range(2)
    ]

    across = [
        (2 * z + 1 - c, 2 * ((z + (1 if c == 0 else -1)) % planes) + c)
        for z in range(planes)
        for c in range(2)
    ]

    def sent(value, pairs):
        return lax.ppermute(value, "tp", pairs)

    tokens = tokens.reshape(rows, width)
    chain_a = sent(tokens, onward)
    chain_b = sent(tokens, across)
    fresh = new_token[:, 0]
    other_fresh = sent(new_token, partner)[:, 0]
    padding = jnp.zeros((EXTRA - prompts, width), new_token.dtype)
    new_pair = jnp.concatenate(
        [
            jnp.where(core == 0, fresh, other_fresh),
            padding,
            jnp.where(core == 0, other_fresh, fresh),
            padding,
        ],
        axis=0,
    )
    new_first = sent(new_pair, onward)
    a_list, b_list = [tokens, chain_a], [None, chain_b]
    new_list = [new_first]
    chain_a, first_position = lax.optimization_barrier((chain_a, own_index * span_len))
    a_list[1] = chain_a
    cosine, sine = tables(first_position, span_len, groups * span_len, heads)
    new_first, cosine, sine = lax.optimization_barrier((new_first, cosine, sine))
    chain_b = jnp.concatenate([chain_b, new_first], axis=0)
    key_weight, value_weight, chain_b = lax.optimization_barrier(
        (key_weight, value_weight, chain_b)
    )
    main_weights = beside(key_weight, value_weight)
    other_weights = sent(main_weights, partner)
    b_list[0] = sent(tokens, partner)
    for _ in range(2, reach):
        chain_a = sent(chain_a, onward)
        chain_b = sent(chain_b, onward)
        a_list.append(chain_a)
        b_list.append(chain_b)
        new_list.append(chain_b[rows:])
    down = [(2 * z + 1, 2 * ((z - 1) % planes) + 1) for z in range(planes)]
    inward = [(2 * z + 1, 2 * z) for z in range(planes)]
    up = [(2 * z, 2 * ((z + 1) % planes)) for z in range(planes)]
    last_up = sent(chain_a, up)
    last_down = sent(chain_a, down)
    last_b = sent(chain_b, down)
    far_new = sent(new_list[-1], onward)
    mine_new = jnp.concatenate(new_list[: reach - 3], axis=0)
    theirs_new = sent(mine_new, partner)
    near_list = new_list[reach - 3 :]
    near_new = jnp.concatenate(near_list, axis=0)

    sums = ()
    for offsets in ((1, 2), (0, 3, 4), (5, 6), (7,)):
        sums = ring_sums(
            offsets,
            span_len,
            place,
            main_weights,
            other_weights,
            [a_list[k] for k in offsets],
            [b_list[k] for k in offsets],
            sums,
            near_list if offsets[-1] == reach - 1 else (),
        )
    own, other = sums

    arrived = sent(other, partner)
    passed_a = sent(last_down, inward)

    messages, own_term = span_states(
        prompts,
        groups,
        inner,
        place,
        own,
        arrived,
        new_pair,
        mine_new,
        near_new,
        theirs_new,
        far_new,
        last_up,
        last_down,
        last_b,
        passed_a,
        main_weights,
        query_weight,
        cosine,
        sine,
        decay=log_decay,
    )
    arrived = lax.all_to_all(messages, "sp", split_axis=0, concat_axis=0, tiled=True)
    return tuple(finish(arrived, own_term, prompts, heads, HD // groups))


def solution(mesh):
    return jax.shard_map(
        body,
        mesh=mesh,
        in_specs=(
            P(None, "sp", "tp"),
            P(None, None, "tp"),
            P(None, "tp"),
            P(None, "tp"),
            P(None, "tp"),
            P("tp"),
        ),
        out_specs=(P(None, "tp", "sp", None), P(None, "tp")),
        check_vma=False,
    )
```

```python
import functools

import jax
import jax.numpy as jnp
from jax import lax
from jax.experimental import pallas as pl
from jax.experimental.pallas import tpu as pltpu
from jax.sharding import PartitionSpec as P

HD = 64
EPS = 1e-05
EXTRA = 16


def swap_halves(values):
    lanes = values.shape[-1]
    lane = lax.broadcasted_iota(jnp.int32, values.shape, len(values.shape) - 1)
    quarter = HD // 2
    back = pltpu.roll(values, lanes - quarter, len(values.shape) - 1)
    ahead = pltpu.roll(values, quarter, len(values.shape) - 1)
    return jnp.where(lane % HD < quarter, back, ahead)


def beside_kernel(left_ref, right_ref, out_ref):
    width = left_ref.shape[1]
    out_ref[:, :width] = left_ref[...]
    out_ref[:, width:] = right_ref[...]


def beside(left, right):
    rows, width = left.shape
    whole = pl.BlockSpec(memory_space=pltpu.VMEM)
    return pl.pallas_call(
        beside_kernel,
        in_specs=[whole, whole],
        out_specs=whole,
        out_shape=jax.ShapeDtypeStruct((rows, 2 * width), left.dtype),
        compiler_params=pltpu.CompilerParams(vmem_limit_bytes=6 * 1024 * 1024),
        cost_estimate=pl.CostEstimate(flops=10**8, bytes_accessed=0, transcendentals=0),
        name="beside",
    )(left, right)


def row_block(place_ref, offset):
    planes = place_ref[3]
    toward = 1 - 2 * place_ref[1]
    return lax.rem(place_ref[0] - offset * toward + planes, planes)


def at_rows(block, width):
    return pl.ds(pl.multiple_of(block * width, width), width)


def stacked(place_ref, weight_ref, offsets, width):
    core = place_ref[1]
    blocks = []
    for offset in offsets:
        plane = row_block(place_ref, offset)
        blocks.append(weight_ref[at_rows(2 * plane + core, width), :])
        blocks.append(weight_ref[at_rows(2 * plane + 1 - core, width), :])
    return jnp.concatenate(blocks, axis=0)


def sums_kernel(offsets, span_len, has_before, place_ref, own_w_ref, other_w_ref, *refs):
    count = len(offsets)
    a_refs, b_refs, rest = refs[:count], refs[count : 2 * count], refs[2 * count :]
    before = rest[:2] if has_before else ()
    own_ref, other_ref, held, landed = rest[len(before) :]
    rows, width = a_refs[0].shape
    core = place_ref[1]
    hops = [i for i in range(count) if offsets[i] > 0]

    copies = []
    for j, i in enumerate(hops):
        plane = row_block(place_ref, offsets[i])
        for side, block in enumerate((2 * plane + core, 2 * plane + 1 - core)):
            slot = 2 * j + side
            copies.append(
                pltpu.make_async_copy(
                    other_w_ref.at[at_rows(block, width), :],
                    held.at[pl.ds(slot * width, width), :],
                    landed.at[slot],
                )
            )
    for copy in copies:
        copy.start()

    def summed(out_ref, earlier, which, weights_of):
        def step(s, carry):
            at = pl.ds(pl.multiple_of(s * span_len, span_len), span_len)
            pieces = []
            for i in which:
                pieces += [a_refs[i][at, :], b_refs[i][at, :]]
            both = jnp.concatenate(pieces, axis=1)
            part = jnp.dot(both, weights_of(), preferred_element_type=jnp.float32)
            if earlier is not None:
                part += earlier[at, :]
            out_ref[at, :] = part
            return carry

        lax.fori_loop(0, rows // span_len, step, 0)

    summed(
        own_ref,
        before[0] if before else None,
        list(range(count)),
        lambda: stacked(place_ref, own_w_ref, offsets, width),
    )
    for copy in copies:
        copy.wait()
    summed(other_ref, before[1] if before else None, hops, lambda: held[...])


def ring_sums(offsets, span_len, place, own_weights, other_weights, a_list, b_list, before):
    rows, width = a_list[0].shape
    inner = own_weights.shape[1]
    whole = pl.BlockSpec(memory_space=pltpu.VMEM)
    operands = [*a_list, *b_list, *before]
    blocks = 2 * sum(1 for offset in offsets if offset > 0)
    flops = 2 * rows * 2 * inner * 2 * width * len(offsets)
    return pl.pallas_call(
        functools.partial(sums_kernel, offsets, span_len, bool(before)),
        in_specs=[
            pl.BlockSpec(memory_space=pltpu.SMEM),
            whole,
            pl.BlockSpec(memory_space=pltpu.HBM),
        ]
        + [whole] * len(operands),
        out_specs=[whole, whole],
        out_shape=[jax.ShapeDtypeStruct((rows, inner), jnp.float32)] * 2,
        scratch_shapes=[
            pltpu.VMEM((blocks * width, inner), own_weights.dtype),
            pltpu.SemaphoreType.DMA((blocks,)),
        ],
        compiler_params=pltpu.CompilerParams(vmem_limit_bytes=6 * 1024 * 1024),
        cost_estimate=pl.CostEstimate(flops=flops, bytes_accessed=0, transcendentals=0),
        name="ring_sums",
    )(place, own_weights, other_weights, *operands)


def pair(ref, start):
    return [ref[start : start + EXTRA, :], ref[start + EXTRA : start + 2 * EXTRA, :]]


def new_rows_product(place_ref, main_ref, query_w_ref, pieces, order):
    width = pieces[0].shape[1]
    plane_rows = [at_rows(row_block(place_ref, k), 2 * width) for k in order]
    weights = jnp.concatenate(
        [jnp.concatenate([main_ref[at, :], query_w_ref[at, :]], axis=1) for at in plane_rows], axis=0
    )
    entries = jnp.concatenate(pieces, axis=1)
    return jnp.dot(entries, weights, preferred_element_type=jnp.float32)


def new_kernel(place_ref, here_new_ref, mine_new_ref, main_ref, query_w_ref, out_ref):
    pieces = pair(here_new_ref, 0)
    order = [0]
    for k in range(1, mine_new_ref.shape[0] // (2 * EXTRA) + 1):
        pieces += pair(mine_new_ref, (k - 1) * 2 * EXTRA)
        order.append(k)
    out_ref[...] = new_rows_product(place_ref, main_ref, query_w_ref, pieces, order)


def new_sums(place, here_new, mine_new, main_weights, query_weight):
    whole = pl.BlockSpec(memory_space=pltpu.VMEM)
    inner = main_weights.shape[1] + query_weight.shape[1]
    return pl.pallas_call(
        new_kernel,
        in_specs=[pl.BlockSpec(memory_space=pltpu.SMEM)] + [whole] * 4,
        out_specs=whole,
        out_shape=jax.ShapeDtypeStruct((EXTRA, inner), jnp.float32),
        compiler_params=pltpu.CompilerParams(vmem_limit_bytes=6 * 1024 * 1024),
        name="new_sums",
    )(place, here_new, mine_new, main_weights, query_weight)


def state_kernel(
    place_ref,
    rate_ref,
    total_ref,
    arrived_ref,
    early_ref,
    theirs_new_ref,
    last_a_ref,
    last_b_ref,
    main_ref,
    query_w_ref,
    cos_ref,
    sin_ref,
    out_ref,
    own_ref,
):
    rows, width = last_a_ref.shape
    inner = query_w_ref.shape[1]
    groups, out_rows, _ = out_ref.shape
    keep = HD // groups
    prompts = out_rows // (keep + 1)
    span_len = rows // prompts
    reach = theirs_new_ref.shape[0] // (2 * EXTRA) + 1
    lane = lax.broadcasted_iota(jnp.int32, (HD, inner), 1)
    row_lane = lax.broadcasted_iota(jnp.int32, (1, inner), 1)
    lane_decay = jnp.full((1, inner), rate_ref[0], jnp.float32)
    for h in range(1, inner // HD):
        lane_decay = jnp.where(row_lane // HD == h, rate_ref[h], lane_decay)
    distance = ((groups - 1 - place_ref[2]) * span_len).astype(jnp.float32)
    carried = jnp.exp(lane_decay * distance)
    one = jnp.exp(lane_decay)
    to_end = lax.broadcasted_iota(jnp.int32, (span_len, inner), 0)
    decay = jnp.exp((span_len - 1 - to_end).astype(jnp.float32) * lane_decay)

    pieces, order = [], []
    for k in range(1, reach):
        pieces += pair(theirs_new_ref, (k - 1) * 2 * EXTRA)
        order.append(-k)
    pieces += pair(last_b_ref, rows)
    order.append(reach)
    fresh = early_ref[...] + new_rows_product(place_ref, main_ref, query_w_ref, pieces, order)
    new_cos = cos_ref[span_len : span_len + 1, :]
    new_sin = sin_ref[span_len : span_len + 1, :]
    new_key = fresh[:, :inner]
    new_key = new_key * new_cos + swap_halves(new_key) * new_sin
    new_key = new_key.astype(jnp.bfloat16).astype(jnp.float32)
    new_value = fresh[:, inner : 2 * inner].astype(jnp.bfloat16).astype(jnp.float32)
    query = fresh[:, 2 * inner :]
    query = (query * new_cos + swap_halves(query) * new_sin) * (HD**0.5)
    query = query.astype(jnp.bfloat16).astype(jnp.float32)
    products = query * new_key
    new_lane = lax.broadcasted_iota(jnp.int32, products.shape, 1)
    score = jnp.zeros_like(products)
    for h in range(inner // HD):
        here = new_lane // HD == h
        score = jnp.where(
            here, jnp.sum(jnp.where(here, products, 0.0), axis=1, keepdims=True), score
        )
    own_ref[...] = score * new_value
    columns = jnp.transpose(query)

    last_weights = stacked(place_ref, main_ref, [reach], width)
    cosine = cos_ref[:span_len, :]
    sine = sin_ref[:span_len, :]
    for s in range(prompts):
        at = pl.ds(s * span_len, span_len)
        last = jnp.concatenate([last_a_ref[at, :], last_b_ref[at, :]], axis=1)
        total = total_ref[at, :] + arrived_ref[at, :]
        total += jnp.dot(last, last_weights, preferred_element_type=jnp.float32)
        keys = total[:, :inner]
        values = total[:, inner:].astype(jnp.bfloat16)
        keys = (keys * cosine + swap_halves(keys) * sine).astype(jnp.bfloat16)
        weighted = (keys.astype(jnp.float32) * decay).astype(jnp.bfloat16)
        full = lax.dot_general(
            weighted, values, (((0,), (0,)), ((), ())), preferred_element_type=jnp.float32
        )
        state = jnp.where(lane < HD, full[:HD], full[HD:]) * carried
        column = jnp.where(lane < HD, columns[:HD, s : s + 1], columns[HD:, s : s + 1])
        read = jnp.sum(state * column, axis=0, keepdims=True) * one
        for g in range(groups):
            out_ref[g, s * keep : (s + 1) * keep, :] = state[g * keep : (g + 1) * keep]
            out_ref[g, prompts * keep + s : prompts * keep + s + 1, :] = read


def span_states(prompts, groups, inner, place, *operands, decay):
    keep = HD // groups
    whole = pl.BlockSpec(memory_space=pltpu.VMEM)
    return pl.pallas_call(
        state_kernel,
        in_specs=[pl.BlockSpec(memory_space=pltpu.SMEM)] * 2 + [whole] * len(operands),
        out_specs=[whole, whole],
        out_shape=[
            jax.ShapeDtypeStruct((groups, prompts * (keep + 1), inner), jnp.float32),
            jax.ShapeDtypeStruct((EXTRA, inner), jnp.float32),
        ],
        compiler_params=pltpu.CompilerParams(vmem_limit_bytes=8 * 1024 * 1024),
        name="span_states",
    )(place, decay, *operands)


def finish_kernel(arrived_ref, own_ref, state_ref, read_ref):
    total = jnp.sum(arrived_ref[...], axis=0)
    prompts, heads, keep, _ = state_ref.shape
    for s in range(prompts):
        for h in range(heads):
            state_ref[s, h] = total[s * keep : (s + 1) * keep, h * HD : (h + 1) * HD].astype(
                jnp.bfloat16
            )
    raw = total[prompts * keep :] + own_ref[:prompts, :]
    lane = lax.broadcasted_iota(jnp.int32, raw.shape, 1)

    def per_head(values):
        result = jnp.zeros_like(values)
        for h in range(heads):
            here = lane // HD == h
            mean = jnp.sum(jnp.where(here, values, 0.0), axis=1, keepdims=True) / HD
            result = jnp.where(here, mean, result)
        return result

    centered = raw - per_head(raw)
    spread = per_head(centered * centered)
    read_ref[...] = (centered * lax.rsqrt(spread + EPS)).astype(jnp.bfloat16)


def finish(arrived, own_term, prompts, heads, keep):
    inner = own_term.shape[1]
    whole = pl.BlockSpec(memory_space=pltpu.VMEM)
    return pl.pallas_call(
        finish_kernel,
        in_specs=[whole, whole],
        out_specs=[whole, whole],
        out_shape=[
            jax.ShapeDtypeStruct((prompts, heads, keep, HD), jnp.bfloat16),
            jax.ShapeDtypeStruct((prompts, inner), jnp.bfloat16),
        ],
        compiler_params=pltpu.CompilerParams(vmem_limit_bytes=4 * 1024 * 1024),
        name="finish",
    )(arrived, own_term)


def tables(first_position, span_len, new_position, heads):
    quarter = HD // 2
    lane = jnp.arange(heads * HD, dtype=jnp.int32)
    inverse = 10000.0 ** (-(lane % quarter).astype(jnp.float32) / quarter)
    row = jnp.arange(span_len + 8, dtype=jnp.int32)
    position = jnp.where(row < span_len, first_position + row, new_position).astype(jnp.float32)
    angles = position[:, None] * inverse[None, :]
    key_scale = HD ** (-0.5)
    sign = jnp.where(lane % HD < quarter, -key_scale, key_scale)
    return jnp.cos(angles) * key_scale, jnp.sin(angles) * sign[None, :]


def body(tokens, new_token, query_weight, key_weight, value_weight, log_decay):
    prompts, span_len, width = tokens.shape
    heads = log_decay.shape[0]
    inner = heads * HD
    groups = lax.axis_size("sp")
    own_index = lax.axis_index("sp")
    tp_index = lax.axis_index("tp")
    planes = lax.axis_size("tp") // 2
    reach = planes // 2
    plane = tp_index // 2
    core = tp_index % 2
    rows = prompts * span_len
    place = jnp.stack([plane, core, own_index, jnp.int32(planes)]).astype(jnp.int32)

    partner = [(i, i ^ 1) for i in range(2 * planes)]
    onward = [
        (2 * z + c, 2 * ((z + (1 if c == 0 else -1)) % planes) + c)
        for z in range(planes)
        for c in range(2)
    ]

    across = [
        (2 * z + 1 - c, 2 * ((z + (1 if c == 0 else -1)) % planes) + c)
        for z in range(planes)
        for c in range(2)
    ]

    def sent(value, pairs):
        return lax.ppermute(value, "tp", pairs)

    tokens = tokens.reshape(rows, width)
    chain_a = sent(tokens, onward)
    chain_b = sent(tokens, across)
    fresh = new_token[:, 0]
    other_fresh = sent(new_token, partner)[:, 0]
    padding = jnp.zeros((EXTRA - prompts, width), new_token.dtype)
    new_pair = jnp.concatenate(
        [
            jnp.where(core == 0, fresh, other_fresh),
            padding,
            jnp.where(core == 0, other_fresh, fresh),
            padding,
        ],
        axis=0,
    )
    new_first = sent(new_pair, onward)
    a_list, b_list = [tokens, chain_a], [None, chain_b]
    new_list = [new_first]
    chain_a, first_position = lax.optimization_barrier((chain_a, own_index * span_len))
    a_list[1] = chain_a
    cosine, sine = tables(first_position, span_len, groups * span_len, heads)
    new_first, cosine, sine = lax.optimization_barrier((new_first, cosine, sine))
    chain_b = jnp.concatenate([chain_b, new_first], axis=0)
    key_weight, value_weight, chain_b = lax.optimization_barrier(
        (key_weight, value_weight, chain_b)
    )
    main_weights = beside(key_weight, value_weight)
    other_weights = sent(main_weights, partner)
    b_list[0] = sent(tokens, partner)
    for _ in range(2, reach + 1):
        chain_a = sent(chain_a, onward)
        chain_b = sent(chain_b, onward)
        a_list.append(chain_a)
        b_list.append(chain_b)
        new_list.append(chain_b[rows:])
    sums = ()
    for offsets in ((1, 2), (0, 3, 4), (5, 6), (7,)):
        sums = ring_sums(
            offsets,
            span_len,
            place,
            main_weights,
            other_weights,
            [a_list[k] for k in offsets],
            [b_list[k] for k in offsets],
            sums,
        )
    own, other = sums

    arrived = sent(other, partner)
    mine_new = jnp.concatenate(new_list[:-1], axis=0)
    theirs_new = sent(mine_new, partner)

    early = new_sums(place, new_pair, mine_new, main_weights, query_weight)
    messages, own_term = span_states(
        prompts,
        groups,
        inner,
        place,
        own,
        arrived,
        early,
        theirs_new,
        a_list[-1],
        b_list[-1],
        main_weights,
        query_weight,
        cosine,
        sine,
        decay=log_decay,
    )
    arrived = lax.all_to_all(messages, "sp", split_axis=0, concat_axis=0, tiled=True)
    return tuple(finish(arrived, own_term, prompts, heads, HD // groups))


def solution(mesh):
    return jax.shard_map(
        body,
        mesh=mesh,
        in_specs=(
            P(None, "sp", "tp"),
            P(None, None, "tp"),
            P(None, "tp"),
            P(None, "tp"),
            P(None, "tp"),
            P("tp"),
        ),
        out_specs=(P(None, "tp", "sp", None), P(None, "tp")),
        check_vma=False,
    )
```

```python
import functools

import jax
import jax.numpy as jnp
from jax import lax
from jax.experimental import pallas as pl
from jax.experimental.pallas import tpu as pltpu
from jax.sharding import PartitionSpec as P

HD = 64
EPS = 1e-05
EXTRA = 16


def swap_halves(values):
    lanes = values.shape[-1]
    lane = lax.broadcasted_iota(jnp.int32, values.shape, len(values.shape) - 1)
    quarter = HD // 2
    back = pltpu.roll(values, lanes - quarter, len(values.shape) - 1)
    ahead = pltpu.roll(values, quarter, len(values.shape) - 1)
    return jnp.where(lane % HD < quarter, back, ahead)


def beside_kernel(left_ref, right_ref, out_ref):
    width = left_ref.shape[1]
    out_ref[:, :width] = left_ref[...]
    out_ref[:, width:] = right_ref[...]


def beside(left, right):
    rows, width = left.shape
    whole = pl.BlockSpec(memory_space=pltpu.VMEM)
    return pl.pallas_call(
        beside_kernel,
        in_specs=[whole, whole],
        out_specs=whole,
        out_shape=jax.ShapeDtypeStruct((rows, 2 * width), left.dtype),
        compiler_params=pltpu.CompilerParams(vmem_limit_bytes=6 * 1024 * 1024),
        cost_estimate=pl.CostEstimate(flops=10**8, bytes_accessed=0, transcendentals=0),
        name="beside",
    )(left, right)


def row_block(place_ref, offset):
    planes = place_ref[3]
    toward = 1 - 2 * place_ref[1]
    return lax.rem(place_ref[0] - offset * toward + planes, planes)


def at_rows(block, width):
    return pl.ds(pl.multiple_of(block * width, width), width)


def stacked(place_ref, weight_ref, offsets, width):
    core = place_ref[1]
    blocks = []
    for offset in offsets:
        plane = row_block(place_ref, offset)
        blocks.append(weight_ref[at_rows(2 * plane + core, width), :])
        blocks.append(weight_ref[at_rows(2 * plane + 1 - core, width), :])
    return jnp.concatenate(blocks, axis=0)


def sums_kernel(offsets, span_len, has_before, place_ref, own_w_ref, other_w_ref, *refs):
    count = len(offsets)
    a_refs, b_refs, rest = refs[:count], refs[count : 2 * count], refs[2 * count :]
    before = rest[:2] if has_before else ()
    own_ref, other_ref, held, landed = rest[len(before) :]
    rows, width = a_refs[0].shape
    core = place_ref[1]
    hops = [i for i in range(count) if offsets[i] > 0]

    copies = []
    for j, i in enumerate(hops):
        plane = row_block(place_ref, offsets[i])
        for side, block in enumerate((2 * plane + core, 2 * plane + 1 - core)):
            slot = 2 * j + side
            copies.append(
                pltpu.make_async_copy(
                    other_w_ref.at[at_rows(block, width), :],
                    held.at[pl.ds(slot * width, width), :],
                    landed.at[slot],
                )
            )
    for copy in copies:
        copy.start()

    def summed(out_ref, earlier, which, weights_of):
        def step(s, carry):
            at = pl.ds(pl.multiple_of(s * span_len, span_len), span_len)
            pieces = []
            for i in which:
                pieces += [a_refs[i][at, :], b_refs[i][at, :]]
            both = jnp.concatenate(pieces, axis=1)
            part = jnp.dot(both, weights_of(), preferred_element_type=jnp.float32)
            if earlier is not None:
                part += earlier[at, :]
            out_ref[at, :] = part
            return carry

        lax.fori_loop(0, rows // span_len, step, 0)

    summed(
        own_ref,
        before[0] if before else None,
        list(range(count)),
        lambda: stacked(place_ref, own_w_ref, offsets, width),
    )
    for copy in copies:
        copy.wait()
    summed(other_ref, before[1] if before else None, hops, lambda: held[...])


def ring_sums(offsets, span_len, place, own_weights, other_weights, a_list, b_list, before):
    rows, width = a_list[0].shape
    inner = own_weights.shape[1]
    whole = pl.BlockSpec(memory_space=pltpu.VMEM)
    operands = [*a_list, *b_list, *before]
    blocks = 2 * sum(1 for offset in offsets if offset > 0)
    flops = 2 * rows * 2 * inner * 2 * width * len(offsets)
    return pl.pallas_call(
        functools.partial(sums_kernel, offsets, span_len, bool(before)),
        in_specs=[
            pl.BlockSpec(memory_space=pltpu.SMEM),
            whole,
            pl.BlockSpec(memory_space=pltpu.HBM),
        ]
        + [whole] * len(operands),
        out_specs=[whole, whole],
        out_shape=[jax.ShapeDtypeStruct((rows, inner), jnp.float32)] * 2,
        scratch_shapes=[
            pltpu.VMEM((blocks * width, inner), own_weights.dtype),
            pltpu.SemaphoreType.DMA((blocks,)),
        ],
        compiler_params=pltpu.CompilerParams(vmem_limit_bytes=6 * 1024 * 1024),
        cost_estimate=pl.CostEstimate(flops=flops, bytes_accessed=0, transcendentals=0),
        name="ring_sums",
    )(place, own_weights, other_weights, *operands)


def pair(ref, start):
    return [ref[start : start + EXTRA, :], ref[start + EXTRA : start + 2 * EXTRA, :]]


def new_rows_product(place_ref, main_ref, query_w_ref, pieces, order):
    width = pieces[0].shape[1]
    plane_rows = [at_rows(row_block(place_ref, k), 2 * width) for k in order]
    weights = jnp.concatenate(
        [jnp.concatenate([main_ref[at, :], query_w_ref[at, :]], axis=1) for at in plane_rows], axis=0
    )
    entries = jnp.concatenate(pieces, axis=1)
    return jnp.dot(entries, weights, preferred_element_type=jnp.float32)


def lane_rates(rate_ref, inner):
    row_lane = lax.broadcasted_iota(jnp.int32, (1, inner), 1)
    lane_decay = jnp.full((1, inner), rate_ref[0], jnp.float32)
    for h in range(1, inner // HD):
        lane_decay = jnp.where(row_lane // HD == h, rate_ref[h], lane_decay)
    return lane_decay


def new_kernel(
    place_ref, rate_ref, here_new_ref, mine_new_ref, main_ref, query_w_ref, out_ref, decay_ref
):
    span_len, inner = decay_ref.shape
    to_end = lax.broadcasted_iota(jnp.int32, (span_len, inner), 0)
    to_end = (span_len - 1 - to_end).astype(jnp.float32)
    decay_ref[...] = jnp.exp(to_end * lane_rates(rate_ref, inner))
    pieces = pair(here_new_ref, 0)
    order = [0]
    for k in range(1, mine_new_ref.shape[0] // (2 * EXTRA) + 1):
        pieces += pair(mine_new_ref, (k - 1) * 2 * EXTRA)
        order.append(k)
    out_ref[...] = new_rows_product(place_ref, main_ref, query_w_ref, pieces, order)


def new_sums(place, decay, span_len, here_new, mine_new, main_weights, query_weight):
    whole = pl.BlockSpec(memory_space=pltpu.VMEM)
    inner = main_weights.shape[1] + query_weight.shape[1]
    return pl.pallas_call(
        new_kernel,
        in_specs=[pl.BlockSpec(memory_space=pltpu.SMEM)] * 2 + [whole] * 4,
        out_specs=[whole, whole],
        out_shape=[
            jax.ShapeDtypeStruct((EXTRA, inner), jnp.float32),
            jax.ShapeDtypeStruct((span_len, query_weight.shape[1]), jnp.float32),
        ],
        compiler_params=pltpu.CompilerParams(vmem_limit_bytes=6 * 1024 * 1024),
        name="new_sums",
    )(place, decay, here_new, mine_new, main_weights, query_weight)


def state_kernel(
    place_ref,
    rate_ref,
    total_ref,
    arrived_ref,
    early_ref,
    decay_ref,
    theirs_new_ref,
    last_a_ref,
    last_b_ref,
    main_ref,
    query_w_ref,
    cos_ref,
    sin_ref,
    out_ref,
    own_ref,
):
    rows, width = last_a_ref.shape
    inner = query_w_ref.shape[1]
    groups, out_rows, _ = out_ref.shape
    keep = HD // groups
    prompts = out_rows // (keep + 1)
    span_len = rows // prompts
    reach = theirs_new_ref.shape[0] // (2 * EXTRA) + 1
    lane = lax.broadcasted_iota(jnp.int32, (HD, inner), 1)
    lane_decay = lane_rates(rate_ref, inner)
    distance = ((groups - 1 - place_ref[2]) * span_len).astype(jnp.float32)
    carried = jnp.exp(lane_decay * distance)
    one = jnp.exp(lane_decay)
    decay = decay_ref[...]

    pieces, order = [], []
    for k in range(1, reach):
        pieces += pair(theirs_new_ref, (k - 1) * 2 * EXTRA)
        order.append(-k)
    pieces += pair(last_b_ref, rows)
    order.append(reach)
    fresh = early_ref[...] + new_rows_product(place_ref, main_ref, query_w_ref, pieces, order)
    new_cos = cos_ref[span_len : span_len + 1, :]
    new_sin = sin_ref[span_len : span_len + 1, :]
    new_key = fresh[:, :inner]
    new_key = new_key * new_cos + swap_halves(new_key) * new_sin
    new_key = new_key.astype(jnp.bfloat16).astype(jnp.float32)
    new_value = fresh[:, inner : 2 * inner].astype(jnp.bfloat16).astype(jnp.float32)
    query = fresh[:, 2 * inner :]
    query = (query * new_cos + swap_halves(query) * new_sin) * (HD**0.5)
    query = query.astype(jnp.bfloat16).astype(jnp.float32)
    products = query * new_key
    new_lane = lax.broadcasted_iota(jnp.int32, products.shape, 1)
    score = jnp.zeros_like(products)
    for h in range(inner // HD):
        here = new_lane // HD == h
        score = jnp.where(
            here, jnp.sum(jnp.where(here, products, 0.0), axis=1, keepdims=True), score
        )
    own_ref[...] = score * new_value
    columns = jnp.transpose(query)

    last_weights = stacked(place_ref, main_ref, [reach], width)
    cosine = cos_ref[:span_len, :]
    sine = sin_ref[:span_len, :]
    for s in range(prompts):
        at = pl.ds(s * span_len, span_len)
        last = jnp.concatenate([last_a_ref[at, :], last_b_ref[at, :]], axis=1)
        total = total_ref[at, :] + arrived_ref[at, :]
        total += jnp.dot(last, last_weights, preferred_element_type=jnp.float32)
        keys = total[:, :inner]
        values = total[:, inner:].astype(jnp.bfloat16)
        keys = (keys * cosine + swap_halves(keys) * sine).astype(jnp.bfloat16)
        weighted = (keys.astype(jnp.float32) * decay).astype(jnp.bfloat16)
        full = lax.dot_general(
            weighted, values, (((0,), (0,)), ((), ())), preferred_element_type=jnp.float32
        )
        state = jnp.where(lane < HD, full[:HD], full[HD:]) * carried
        column = jnp.where(lane < HD, columns[:HD, s : s + 1], columns[HD:, s : s + 1])
        read = jnp.sum(state * column, axis=0, keepdims=True) * one
        for g in range(groups):
            out_ref[g, s * keep : (s + 1) * keep, :] = state[g * keep : (g + 1) * keep]
            out_ref[g, prompts * keep + s : prompts * keep + s + 1, :] = read


def span_states(prompts, groups, inner, place, *operands, decay):
    keep = HD // groups
    whole = pl.BlockSpec(memory_space=pltpu.VMEM)
    return pl.pallas_call(
        state_kernel,
        in_specs=[pl.BlockSpec(memory_space=pltpu.SMEM)] * 2 + [whole] * len(operands),
        out_specs=[whole, whole],
        out_shape=[
            jax.ShapeDtypeStruct((groups, prompts * (keep + 1), inner), jnp.float32),
            jax.ShapeDtypeStruct((EXTRA, inner), jnp.float32),
        ],
        compiler_params=pltpu.CompilerParams(vmem_limit_bytes=8 * 1024 * 1024),
        name="span_states",
    )(place, decay, *operands)


def finish_kernel(arrived_ref, own_ref, state_ref, read_ref):
    total = jnp.sum(arrived_ref[...], axis=0)
    prompts, heads, keep, _ = state_ref.shape
    for s in range(prompts):
        for h in range(heads):
            state_ref[s, h] = total[s * keep : (s + 1) * keep, h * HD : (h + 1) * HD].astype(
                jnp.bfloat16
            )
    raw = total[prompts * keep :] + own_ref[:prompts, :]
    lane = lax.broadcasted_iota(jnp.int32, raw.shape, 1)

    def per_head(values):
        result = jnp.zeros_like(values)
        for h in range(heads):
            here = lane // HD == h
            mean = jnp.sum(jnp.where(here, values, 0.0), axis=1, keepdims=True) / HD
            result = jnp.where(here, mean, result)
        return result

    centered = raw - per_head(raw)
    spread = per_head(centered * centered)
    read_ref[...] = (centered * lax.rsqrt(spread + EPS)).astype(jnp.bfloat16)


def finish(arrived, own_term, prompts, heads, keep):
    inner = own_term.shape[1]
    whole = pl.BlockSpec(memory_space=pltpu.VMEM)
    return pl.pallas_call(
        finish_kernel,
        in_specs=[whole, whole],
        out_specs=[whole, whole],
        out_shape=[
            jax.ShapeDtypeStruct((prompts, heads, keep, HD), jnp.bfloat16),
            jax.ShapeDtypeStruct((prompts, inner), jnp.bfloat16),
        ],
        compiler_params=pltpu.CompilerParams(vmem_limit_bytes=4 * 1024 * 1024),
        name="finish",
    )(arrived, own_term)


def tables(first_position, span_len, new_position, heads):
    quarter = HD // 2
    lane = jnp.arange(heads * HD, dtype=jnp.int32)
    inverse = 10000.0 ** (-(lane % quarter).astype(jnp.float32) / quarter)
    row = jnp.arange(span_len + 8, dtype=jnp.int32)
    position = jnp.where(row < span_len, first_position + row, new_position).astype(jnp.float32)
    angles = position[:, None] * inverse[None, :]
    key_scale = HD ** (-0.5)
    sign = jnp.where(lane % HD < quarter, -key_scale, key_scale)
    return jnp.cos(angles) * key_scale, jnp.sin(angles) * sign[None, :]


def body(tokens, new_token, query_weight, key_weight, value_weight, log_decay):
    prompts, span_len, width = tokens.shape
    heads = log_decay.shape[0]
    inner = heads * HD
    groups = lax.axis_size("sp")
    own_index = lax.axis_index("sp")
    tp_index = lax.axis_index("tp")
    planes = lax.axis_size("tp") // 2
    reach = planes // 2
    plane = tp_index // 2
    core = tp_index % 2
    rows = prompts * span_len
    place = jnp.stack([plane, core, own_index, jnp.int32(planes)]).astype(jnp.int32)

    partner = [(i, i ^ 1) for i in range(2 * planes)]
    onward = [
        (2 * z + c, 2 * ((z + (1 if c == 0 else -1)) % planes) + c)
        for z in range(planes)
        for c in range(2)
    ]

    across = [
        (2 * z + 1 - c, 2 * ((z + (1 if c == 0 else -1)) % planes) + c)
        for z in range(planes)
        for c in range(2)
    ]

    def sent(value, pairs):
        return lax.ppermute(value, "tp", pairs)

    tokens = tokens.reshape(rows, width)
    chain_a = sent(tokens, onward)
    chain_b = sent(tokens, across)
    fresh = new_token[:, 0]
    other_fresh = sent(new_token, partner)[:, 0]
    padding = jnp.zeros((EXTRA - prompts, width), new_token.dtype)
    new_pair = jnp.concatenate(
        [
            jnp.where(core == 0, fresh, other_fresh),
            padding,
            jnp.where(core == 0, other_fresh, fresh),
            padding,
        ],
        axis=0,
    )
    new_first = sent(new_pair, onward)
    a_list, b_list = [tokens, chain_a], [None, chain_b]
    new_list = [new_first]
    chain_a, first_position = lax.optimization_barrier((chain_a, own_index * span_len))
    a_list[1] = chain_a
    cosine, sine = tables(first_position, span_len, groups * span_len, heads)
    new_first, cosine, sine = lax.optimization_barrier((new_first, cosine, sine))
    chain_b = jnp.concatenate([chain_b, new_first], axis=0)
    key_weight, value_weight, chain_b = lax.optimization_barrier(
        (key_weight, value_weight, chain_b)
    )
    main_weights = beside(key_weight, value_weight)
    other_weights = sent(main_weights, partner)
    b_list[0] = sent(tokens, partner)
    for _ in range(2, reach + 1):
        chain_a = sent(chain_a, onward)
        chain_b = sent(chain_b, onward)
        a_list.append(chain_a)
        b_list.append(chain_b)
        new_list.append(chain_b[rows:])
    sums = ()
    for offsets in ((1, 2), (0, 3, 4), (5, 6), (7,)):
        sums = ring_sums(
            offsets,
            span_len,
            place,
            main_weights,
            other_weights,
            [a_list[k] for k in offsets],
            [b_list[k] for k in offsets],
            sums,
        )
    own, other = sums

    arrived = sent(other, partner)
    mine_new = jnp.concatenate(new_list[:-1], axis=0)
    theirs_new = sent(mine_new, partner)

    early = new_sums(
        place, log_decay, span_len, new_pair, mine_new, main_weights, query_weight
    )
    messages, own_term = span_states(
        prompts,
        groups,
        inner,
        place,
        own,
        arrived,
        *early,
        theirs_new,
        a_list[-1],
        b_list[-1],
        main_weights,
        query_weight,
        cosine,
        sine,
        decay=log_decay,
    )
    arrived = lax.all_to_all(messages, "sp", split_axis=0, concat_axis=0, tiled=True)
    return tuple(finish(arrived, own_term, prompts, heads, HD // groups))


def solution(mesh):
    return jax.shard_map(
        body,
        mesh=mesh,
        in_specs=(
            P(None, "sp", "tp"),
            P(None, None, "tp"),
            P(None, "tp"),
            P(None, "tp"),
            P(None, "tp"),
            P("tp"),
        ),
        out_specs=(P(None, "tp", "sp", None), P(None, "tp")),
        check_vma=False,
    )
```
